32 devices in a mesh: sp: 8 (over z, x), tp: 4 (over y, core).
Axes of the slice: x: 2, y: 2, z: 4, core: 2. Of those that a mesh axis runs over, the one named last changes fastest.
Arguments:
- query_logits: bfloat16 [4096, 4096], P('sp', 'tp'), may hold values from -6 to 6
- forget_logits: bfloat16 [4096, 4096], P('sp', 'tp'), may hold values from -6 to 6
- value_inputs: bfloat16 [4096, 4096], P('sp', 'tp'), may hold values from -16 to 16
- output_gate_logits: bfloat16 [4096, 4096], P('sp', 'tp'), may hold values from -6 to 6
- forget_floor_gap: float32 [4096], replicated, may hold values from 2.4414063e-05 to 0.1
- surge_log_decay: float32 [32, 4096], P('tp', 'sp'), may hold values from -0.7 to 0
- head_norm_gain: float32 [128], replicated, may hold values from 0.1 to 1.9
- output_matrix: bfloat16 [4096, 4096], P('sp', 'tp'), may hold values from -1.25 to 1.25
- branch_norm_gain: float32 [4096], replicated, may hold values from 0.1 to 1.9
- residual: bfloat16 [4096, 4096], P('sp', 'tp'), may hold values from -6 to 6
Outputs:
- output: bfloat16 [4096, 4096], P('sp', 'tp')
The draws below stay inside these ranges and needn't reach their ends.
All inputs are finite; a program needn't handle non-finite values.
Results may differ from the reference program's by a relative error of at most 0.005.
Values may be sent and summed in bfloat16 or wider, within the bound.
No kernel may reach another device: no remote copies, remote signals or barrier semaphores. Data moves between devices by JAX's collectives and lax.ppermute only.
A program may use at most 128 MiB of HBM per device.

```python
import math
import jax
import jax.numpy as jnp
from jax import lax

HEAD_DIM = 128
HEAD_TOTAL = 32
D = 4096
BLOCK_SPAN = 64
TOK_DEV = 512
TOKEN_TOTAL = 4096


surge_count = 3


def draw_forget_logits(key, part):
    leading_item, second = jax.random.split(key, 2)
    width = HEAD_TOTAL * HEAD_DIM
    offsets = jax.random.uniform(second, (TOKEN_TOTAL // TOK_DEV, 1, 1), jnp.float32, -1.5, 1.5)
    base = jnp.clip(jax.random.normal(leading_item, (TOKEN_TOTAL, width), jnp.float32), -4.0, 4.0)
    shifted = base.reshape(TOKEN_TOTAL // TOK_DEV, TOK_DEV, width) + offsets
    return shifted.reshape(TOKEN_TOTAL, width).astype(jnp.bfloat16)


def draw_forget_floor_gap(key, part):
    leading_item, second, third = jax.random.split(key, 3)
    share = 0.5
    quick = jax.random.uniform(leading_item, (HEAD_TOTAL, 1), jnp.float32) < share
    slow_gap = jax.random.uniform(second, (HEAD_TOTAL, HEAD_DIM), jnp.float32, 0.1, 0.6) / TOKEN_TOTAL
    quick_gap = jnp.exp(jax.random.uniform(third, (HEAD_TOTAL, HEAD_DIM), jnp.float32, math.log(0.03), math.log(0.1)))
    return jnp.where(quick, quick_gap, slow_gap).reshape(HEAD_TOTAL * HEAD_DIM)


def draw_surge_log_decay(key, part):
    leading_item, second = jax.random.split(key, 2)
    position_grid = jax.random.randint(leading_item, (HEAD_TOTAL, surge_count), 0, TOKEN_TOTAL)
    hits = jnp.any(jnp.arange(TOKEN_TOTAL)[None, :, None] == position_grid[:, None, :], axis=2)
    amounts = jnp.log(jax.random.uniform(second, (HEAD_TOTAL, TOKEN_TOTAL), jnp.float32, 0.5, 0.8))
    return jnp.where(hits, amounts, 0.0).astype(jnp.float32)


def draw_output_matrix(key, part):
    leading_item, second = jax.random.split(key, 2)
    width = HEAD_TOTAL * HEAD_DIM
    limit = 80.0 / math.sqrt(width)
    ramp = jnp.exp(math.log(3.0) * jnp.arange(D).astype(jnp.float32) / D)
    base = jnp.clip(jax.random.normal(leading_item, (width, D), jnp.float32), -4.0, 4.0)
    column_scale = ramp * jnp.exp(jax.random.uniform(second, (D,), jnp.float32, 0.0, math.log(4.0)))
    values = jnp.clip(base * column_scale / math.sqrt(width), -limit, limit)
    return values.astype(jnp.bfloat16)


def shard_levels(key, extent, cuts, least, top_value):
    def one(dim, parts):
        draws = jax.random.uniform(jax.random.fold_in(jax.random.fold_in(key, 6), dim), (parts,), jnp.float32, least / len(cuts), top_value / len(cuts))
        return jnp.repeat(jnp.exp(draws), extent[dim] // parts).reshape((-1,) + (1,) * (len(extent) - dim - 1))

    loudness = one(*cuts[0])
    for cut in cuts[1:]:
        loudness = loudness * one(*cut)
    return loudness


def noise(own_key, dims, deviation, reach, cuts=(), kind=jnp.bfloat16):
    values = jax.random.normal(own_key, dims, jnp.float32) * deviation
    if len(cuts) > 0:
        values = shard_levels(own_key, dims, cuts, -0.22, 0.18) * values
    return jnp.clip(values, min=-reach, max=reach).astype(kind)


def setup_inputs(seed: int = 0) -> dict:
    arg_keys = jax.random.split(jax.random.key(seed), 11)
    return {
        "query_logits": noise(arg_keys[0], (TOKEN_TOTAL, HEAD_TOTAL * HEAD_DIM), 1.0, 6.0, ((0, 8), (1, 4))),
        "forget_logits": draw_forget_logits(jax.random.fold_in(arg_keys[10], 71), 0),
        "value_inputs": noise(arg_keys[2], (TOKEN_TOTAL, HEAD_TOTAL * HEAD_DIM), 4.0, 16.0, ((0, 8), (1, 4))),
        "output_gate_logits": noise(arg_keys[3], (TOKEN_TOTAL, HEAD_TOTAL * HEAD_DIM), 1.0, 6.0, ((0, 8), (1, 4))),
        "forget_floor_gap": draw_forget_floor_gap(jax.random.fold_in(arg_keys[10], 71), 0),
        "surge_log_decay": draw_surge_log_decay(jax.random.fold_in(arg_keys[10], 71), 0),
        "head_norm_gain": jnp.clip(1.0 + 0.18 * jax.random.normal(arg_keys[6], (HEAD_DIM,), jnp.float32), 0.1, 1.9),
        "output_matrix": draw_output_matrix(jax.random.fold_in(arg_keys[10], 71), 0),
        "branch_norm_gain": jnp.clip(1.0 + 0.18 * jax.random.normal(arg_keys[8], (D,), jnp.float32), 0.1, 1.9),
        "residual": noise(arg_keys[9], (TOKEN_TOTAL, D), 1.0, 6.0, ((0, 8), (1, 4))),
    }


epsilon = 1e-06

def block_update(state, queries, keys_in, values_in, running):
    length = running.shape[1]
    middle = length // 2
    anchor = running[:, middle - 1:middle, :]
    ending = running[:, -1:, :]
    causal = jnp.tril(jnp.ones((length, length), dtype=bool))
    highest = lax.Precision.HIGHEST
    inter = jnp.einsum('htd,hde->hte', queries * jnp.exp(running), state, precision=highest)
    scores = jnp.einsum('htd,hsd->hts', queries * jnp.exp(running - anchor), keys_in * jnp.exp(anchor - running), precision=highest)
    intra = jnp.einsum('hts,hse->hte', jnp.where(causal[None], scores, 0.0), values_in, precision=highest)
    new_state = state * jnp.exp(ending[:, 0, :])[:, :, None] + jnp.einsum('hsd,hse->hde', keys_in * jnp.exp(ending - running), values_in, precision=highest)
    return (new_state, inter + intra)

def head_gates(query_logits, forget_logits, value_inputs, gap):
    row_count = query_logits.shape[0]
    head_count = query_logits.shape[1] // HEAD_DIM

    def shaped(array):
        return array.astype(jnp.float32).reshape(row_count, head_count, HEAD_DIM)
    queries = jax.nn.silu(shaped(query_logits)) * HEAD_DIM ** (-0.5)
    keys_in = gap.reshape(head_count, HEAD_DIM) * jax.nn.sigmoid(-shaped(forget_logits))
    values_in = shaped(value_inputs)
    decay_factors = jnp.log1p(-keys_in)
    return (queries, keys_in, values_in, decay_factors)

def gated_norm(heads_out, output_gate_logits, head_norm_gain):
    mean_sq = lax.optimization_barrier(jnp.mean(heads_out * heads_out, axis=-1, keepdims=True))
    gates = jax.nn.silu(output_gate_logits.astype(jnp.float32).reshape(heads_out.shape))
    normed = heads_out * lax.rsqrt(mean_sq + epsilon) * head_norm_gain * gates
    return normed.reshape(heads_out.shape[0], -1).astype(jnp.bfloat16)

def reference(query_logits, forget_logits, value_inputs, output_gate_logits, forget_floor_gap, surge_log_decay, head_norm_gain, output_matrix, branch_norm_gain, residual):
    number_of_blocks = TOKEN_TOTAL // BLOCK_SPAN

    def split_into_blocks(array):
        return array.reshape(number_of_blocks, BLOCK_SPAN, array.shape[1])
    surge_values = jnp.transpose(surge_log_decay).reshape(number_of_blocks, BLOCK_SPAN, HEAD_TOTAL)

    def step_forward(state, input_tuple):
        query_tile_block, forget_gate_block, value_rows_block, output_gate_block, surge_block, residual_block = input_tuple
        queries, keys_in, values_in, decay_factors = head_gates(query_tile_block, forget_gate_block, value_rows_block, forget_floor_gap)
        decay_factors = decay_factors + surge_block[:, :, None]
        running = jnp.cumsum(jnp.transpose(decay_factors, (1, 0, 2)), axis=1)
        new_state, heads_out = block_update(state, jnp.transpose(queries, (1, 0, 2)), jnp.transpose(keys_in, (1, 0, 2)), jnp.transpose(values_in, (1, 0, 2)), running)
        mixed_rows = gated_norm(jnp.transpose(heads_out, (1, 0, 2)), output_gate_block, head_norm_gain)
        projected = lax.optimization_barrier(jnp.dot(mixed_rows, output_matrix, preferred_element_type=jnp.float32).astype(jnp.bfloat16))
        branch = projected.astype(jnp.float32)
        scale = lax.rsqrt(lax.optimization_barrier(jnp.mean(branch * branch, axis=-1, keepdims=True)) + epsilon)
        result = (residual_block.astype(jnp.float32) + branch * scale * branch_norm_gain).astype(jnp.bfloat16)
        return (new_state, result)
    starting_state = jnp.zeros((HEAD_TOTAL, HEAD_DIM, HEAD_DIM), jnp.float32)
    unused_slot, output_list = lax.scan(step_forward, starting_state, (split_into_blocks(query_logits), split_into_blocks(forget_logits), split_into_blocks(value_inputs), split_into_blocks(output_gate_logits), surge_values, split_into_blocks(residual)))
    return output_list.reshape(TOKEN_TOTAL, D)
```

```python
import functools

import jax
import jax.numpy as jnp
from jax import lax
from jax.experimental import pallas as pl
from jax.experimental.pallas import tpu as pltpu
from jax.sharding import PartitionSpec as P

HEAD_DIM = 128
SPAN = 128
EXTRA = 8
epsilon = 1e-06


f32 = jnp.float32
bf16 = jnp.bfloat16
TN = (((0,), (0,)), ((), ()))
NT = (((1,), (1,)), ((), ()))


def dot(a, b, dims=(((1,), (0,)), ((), ()))):
    return lax.dot_general(a, b, dims, preferred_element_type=f32)


def split2(value):
    high = value.astype(bf16)
    return high, (value - high.astype(f32)).astype(bf16)


def input_gate(forget_logits, gap):
    return gap / (1.0 + jnp.exp(forget_logits.astype(f32)))


def states_kernel(forget_ref, value_ref, surge_ref, gap_ref, running_ref, packed_ref):
    head = pl.program_id(0)
    rows = forget_ref.shape[0]
    gates = input_gate(forget_ref[...], gap_ref[0])
    lane = lax.broadcasted_iota(jnp.int32, surge_ref.shape, 1)
    surge = jnp.sum(jnp.where(lane == head, surge_ref[...], 0.0), axis=1, keepdims=True)
    high, low = split2(jnp.log1p(-gates) + surge)
    lower = lax.broadcasted_iota(jnp.int32, (SPAN, 2 * SPAN), 1) % SPAN
    lower = (lower <= lax.broadcasted_iota(jnp.int32, (SPAN, 2 * SPAN), 0)).astype(bf16)
    after = jnp.zeros((1, HEAD_DIM), f32)
    keys = []
    for start in reversed(range(0, rows, SPAN)):
        part = slice(start, start + SPAN)
        running = dot(lower, jnp.concatenate([high[part], low[part]], axis=0))
        running_ref[part, :] = running
        after = after + running[SPAN - 1 :, :]
        keys.append((gates[part] * jnp.exp(after - running)).astype(bf16))
    keys = jnp.concatenate(keys[::-1], axis=0)
    packed_ref[0, :HEAD_DIM, :] = dot(value_ref[...], keys, TN).astype(bf16)
    packed_ref[0, HEAD_DIM:, :] = pack_decay(jnp.exp(after))


def pack_decay(decay):
    first, rest = split2(decay)
    rest32 = decay - first.astype(f32)
    second, third = split2(rest32)
    row = lax.broadcasted_iota(jnp.int32, (EXTRA, decay.shape[-1]), 0)
    rows = [t.astype(f32) for t in (first, second, third)]
    out = jnp.where(row == 0, rows[0], jnp.where(row == 1, rows[1], jnp.where(row == 2, rows[2], 0.0)))
    return out.astype(bf16)


def unpack(ref, head):
    state = ref[head, :HEAD_DIM, :].astype(f32)
    decay = jnp.sum(ref[head, HEAD_DIM:, :].astype(f32), axis=0, keepdims=True)
    return state, decay


def local_kernel(query_ref, forget_ref, value_ref, running_ref, gap_ref, local_ref, reach_ref):
    rows = query_ref.shape[0]
    before = jnp.zeros((1, HEAD_DIM), f32)
    state = None
    row = lax.broadcasted_iota(jnp.int32, (SPAN, SPAN), 0)
    causal = lax.broadcasted_iota(jnp.int32, (SPAN, SPAN), 1) <= row
    for start in range(0, rows, SPAN):
        part = slice(start, start + SPAN)
        logits = query_ref[part, :].astype(f32)
        queries = logits / (1.0 + jnp.exp(-logits)) * HEAD_DIM**-0.5
        gates = input_gate(forget_ref[part, :], gap_ref[0])
        values = value_ref[part, :]
        running = running_ref[part, :]
        anchor = running[SPAN // 2 - 1 : SPAN // 2, :]
        total = running[SPAN - 1 :, :]
        late = (queries * jnp.exp(running - anchor)).astype(bf16)
        early = (gates * jnp.exp(anchor - running)).astype(bf16)
        scores = jnp.where(causal, dot(late, early, NT), 0.0).astype(bf16)
        out = dot(scores, values)
        faded = queries * jnp.exp(running)
        if state is not None:
            out = out + dot(faded.astype(bf16), state.astype(bf16), NT)
        local_ref[part, :] = out
        reach_ref[part, :] = (faded * jnp.exp(before)).astype(bf16)
        if start + SPAN < rows:
            keys = (gates * jnp.exp(total - running)).astype(bf16)
            fresh = dot(values, keys, TN)
            state = fresh if state is None else state * jnp.exp(total) + fresh
            before = before + total


def pair_kernel(odd_ref, own_ref, other_ref, out_ref):
    even = odd_ref[0] == 0
    for head in range(own_ref.shape[0]):
        own, own_decay = unpack(own_ref, head)
        other, other_decay = unpack(other_ref, head)
        mine = jnp.where(even, other_decay, 1.0)
        theirs = jnp.where(even, 1.0, own_decay)
        out_ref[head, :HEAD_DIM, :] = (own * mine + other * theirs).astype(bf16)
        out_ref[head, HEAD_DIM:, :] = pack_decay(own_decay * other_decay)


def combine_kernel(earlier_ref, later_ref, out_ref):
    for head in range(later_ref.shape[0]):
        early, early_decay = unpack(earlier_ref, head)
        late, late_decay = unpack(later_ref, head)
        out_ref[head, :HEAD_DIM, :] = (early * late_decay + late).astype(bf16)
        out_ref[head, HEAD_DIM:, :] = pack_decay(early_decay * late_decay)


def carry_kernel(odd_ref, before_ref, other_ref, out_ref):
    odd = odd_ref[0] == 1
    for head in range(before_ref.shape[0]):
        before, _ = unpack(before_ref, head)
        other, other_decay = unpack(other_ref, head)
        out_ref[head] = jnp.where(odd, before * other_decay + other, before).astype(bf16)


def mix_kernel(local_ref, reach_ref, carried_ref, gate_ref, gain_ref, out_ref):
    heads_out = local_ref[...] + dot(reach_ref[...], carried_ref[0], NT)
    mean_sq = jnp.mean(heads_out * heads_out, axis=1, keepdims=True)
    logits = gate_ref[...].astype(f32)
    gates = logits / (1.0 + jnp.exp(-logits))
    out_ref[...] = (heads_out * lax.rsqrt(mean_sq + epsilon) * gain_ref[...] * gates).astype(bf16)


def project_kernel(slots_ref, order_ref, *refs, n_mixed):
    mixed = refs[:n_mixed]
    rows = refs[n_mixed:-3]
    out_ref, far_ref, table = refs[-3:]

    @pl.when(pl.program_id(0) == 0)
    def _():
        for i, piece in enumerate(mixed):
            table[slots_ref[i]] = piece[...]
        far_ref[...] = table[order_ref[len(rows) // 2]]

    half = rows[0].shape[0]
    total = None
    for i in range(0, len(rows), 2):
        block = order_ref[i // 2]
        for j in range(2):
            part = dot(table[block, :, j * half : (j + 1) * half], rows[i + j][...])
            total = part if total is None else total + part
    out_ref[...] = total


def finish_kernel(piece_ref, first_ref, second_ref, partial_ref, out_ref, square_ref, lanes_ref):
    half = first_ref.shape[0]
    total = partial_ref[...] + dot(piece_ref[:, :half], first_ref[...])
    total = total + dot(piece_ref[:, half:], second_ref[...])
    rounded = total.astype(bf16)
    out_ref[...] = rounded
    wide = rounded.astype(f32)
    squares = wide * wide
    lanes = squares[:, :128]
    for start in range(128, squares.shape[1], 128):
        lanes = lanes + squares[:, start : start + 128]

    @pl.when(pl.program_id(0) == 0)
    def _():
        lanes_ref[...] = lanes

    @pl.when(pl.program_id(0) > 0)
    def _():
        lanes_ref[...] += lanes

    @pl.when(pl.program_id(0) == pl.num_programs(0) - 1)
    def _():
        high, low = split2(lanes_ref[...])
        ones = jnp.ones((8, 128), bf16)
        square_ref[...] = (dot(ones, high, NT) + dot(ones, low, NT))[:1]


def vmem(shape=None):
    return pl.BlockSpec(memory_space=pltpu.VMEM)


def smem():
    return pl.BlockSpec(memory_space=pltpu.SMEM)


def ring_gather(own, axis, ring):
    size = len(ring)
    forward = [(ring[i], ring[(i + 1) % size]) for i in range(size)]
    backward = [(b, a) for a, b in forward]
    half = own.shape[0] // 2
    chunks = {0: (own[:half], own[half:])}
    for step in range(1, size // 2):
        for sign, pairs in ((-1, forward), (1, backward)):
            chunks[sign * step] = [None, None]
        for part in range(2):
            for sign, pairs in ((-1, forward), (1, backward)):
                chunks[sign * step][part] = lax.ppermute(chunks[sign * (step - 1)][part], axis, pairs)
    last = size // 2
    far = (
        lax.ppermute(chunks[-(last - 1)][0], axis, forward),
        lax.ppermute(chunks[last - 1][1], axis, backward),
    )
    return chunks, far


def swap(array, axis, bit):
    size = lax.axis_size(axis)
    return lax.ppermute(array, axis, [(i, i ^ bit) for i in range(size)])


def shift(array, axis, by):
    size = lax.axis_size(axis)
    return lax.ppermute(array, axis, [(i, i + by) for i in range(size - by)])


def carried_state(packed, axis):
    size, position = lax.axis_size(axis), lax.axis_index(axis)
    odd = jnp.reshape(position % 2, (1,)).astype(jnp.int32)
    like = jax.ShapeDtypeStruct(packed.shape, packed.dtype)
    other = swap(packed, axis, 1)
    pair = pl.pallas_call(pair_kernel, out_shape=like, in_specs=[smem(), vmem(), vmem()], out_specs=vmem(), name="pair")(odd, packed, other)
    combine = pl.pallas_call(combine_kernel, out_shape=like, in_specs=[vmem(), vmem()], out_specs=vmem(), name="combine")
    before = shift(pair, axis, 2)
    reach = 2
    while reach < size // 2:
        whole = combine(before, pair)
        before = combine(shift(whole, axis, 2 * reach), before)
        reach *= 2
    heads = packed.shape[0]
    return pl.pallas_call(
        carry_kernel,
        out_shape=jax.ShapeDtypeStruct((heads, HEAD_DIM, HEAD_DIM), bf16),
        in_specs=[smem(), vmem(), vmem()],
        out_specs=vmem(),
        name="carry",
    )(odd, before, other)


def per_device(
    query_logits,
    forget_logits,
    value_inputs,
    output_gate_logits,
    forget_floor_gap,
    surge_log_decay,
    head_norm_gain,
    output_matrix,
    branch_norm_gain,
    residual,
):
    rows, head_cols = query_logits.shape
    heads = head_cols // HEAD_DIM
    sp, tp = lax.axis_size("sp"), lax.axis_size("tp")
    sp_at, tp_at = lax.axis_index("sp"), lax.axis_index("tp")
    width = output_matrix.shape[0] * sp
    out_cols = output_matrix.shape[1]

    ring = list(range(0, sp, 2)) + list(range(1, sp, 2))[::-1]
    ringed = sp <= 8 and sp % tp == 0
    if ringed:
        chunks, far = ring_gather(output_matrix, "sp", ring)
    else:
        whole_weight = lax.all_gather(output_matrix, "sp", axis=0, tiled=True)

    gap = lax.dynamic_slice_in_dim(forget_floor_gap, tp_at * head_cols, head_cols)
    gap = gap.reshape(heads, 1, HEAD_DIM)
    block = pl.BlockSpec((rows, HEAD_DIM), lambda h: (0, h))
    gap_block = pl.BlockSpec((1, 1, HEAD_DIM), lambda h: (h, 0, 0))
    full = jax.ShapeDtypeStruct((rows, head_cols), f32)
    running, packed = pl.pallas_call(
        states_kernel,
        grid=(heads,),
        out_shape=(full, jax.ShapeDtypeStruct((heads, HEAD_DIM + EXTRA, HEAD_DIM), bf16)),
        in_specs=[block, block, pl.BlockSpec((rows, heads), lambda h: (0, 0)), gap_block],
        out_specs=(block, pl.BlockSpec((1, HEAD_DIM + EXTRA, HEAD_DIM), lambda h: (h, 0, 0))),
        name="states",
    )(forget_logits, value_inputs, jnp.transpose(surge_log_decay), gap)

    carried = carried_state(packed, "sp")

    local, reach = pl.pallas_call(
        local_kernel,
        grid=(heads,),
        out_shape=(full, jax.ShapeDtypeStruct((rows, head_cols), bf16)),
        in_specs=[block, block, block, block, gap_block],
        out_specs=(block, block),
        name="local",
    )(query_logits, forget_logits, value_inputs, running, gap)

    def mix(first, count):
        shifted = pl.BlockSpec((rows, HEAD_DIM), lambda h: (0, first + h))
        return pl.pallas_call(
            mix_kernel,
            grid=(count,),
            out_shape=jax.ShapeDtypeStruct((rows, count * HEAD_DIM), bf16),
            in_specs=[
                shifted,
                shifted,
                pl.BlockSpec((1, HEAD_DIM, HEAD_DIM), lambda h: (first + h, 0, 0)),
                shifted,
                pl.BlockSpec((1, HEAD_DIM), lambda h: (0, 0)),
            ],
            out_specs=pl.BlockSpec((rows, HEAD_DIM), lambda h: (0, h)),
            name="mix",
        )(local, reach, carried, output_gate_logits, head_norm_gain.reshape(1, HEAD_DIM))

    parts = sp // tp if ringed else 2
    per = head_cols // parts
    halves = [mix(i * heads // parts, heads // parts) for i in range(parts)]
    pieces = {0: halves}
    bit = tp // 2
    while bit:
        for rel in sorted(pieces):
            pieces[rel ^ bit] = [swap(half, "tp", bit) for half in pieces[rel]]
        bit //= 2
    mixed = [pieces[rel][i] for rel in range(tp) for i in range(parts)]
    source = jnp.stack([(tp_at ^ rel) * parts + i for rel in range(tp) for i in range(parts)])
    source = source.astype(jnp.int32)

    if not ringed:
        ordered = jnp.stack([p for p in mixed])
        slots = jnp.argsort(source)
        all_heads = jnp.concatenate([ordered[slots[i]] for i in range(len(mixed))], axis=1)
        projected = jnp.dot(all_heads, whole_weight, preferred_element_type=f32).astype(bf16)
        wide = lax.optimization_barrier(projected).astype(f32)
        squares = jnp.sum(wide * wide, axis=1)[None]
    else:
        offsets = [0] + [s * k for k in range(1, sp // 2) for s in (-1, 1)] + [sp // 2]
        table = jnp.array(ring, jnp.int32)
        at = jnp.argmax(table == sp_at)
        order = jnp.stack([table[(at + off) % sp] for off in offsets]).astype(jnp.int32)
        tile = 256
        piece = pl.BlockSpec((rows, per), lambda n: (0, 0))
        slab = pl.BlockSpec((per // 2, tile), lambda n: (0, n))
        sheet = pl.BlockSpec((rows, tile), lambda n: (0, n))
        parts_in = [chunk for off in offsets[:-1] for chunk in chunks[off]]
        partial, far_piece = pl.pallas_call(
            functools.partial(project_kernel, n_mixed=len(mixed)),
            grid=(out_cols // tile,),
            out_shape=(
                jax.ShapeDtypeStruct((rows, out_cols), f32),
                jax.ShapeDtypeStruct((rows, per), bf16),
            ),
            in_specs=[smem(), smem()] + [piece] * len(mixed) + [slab] * len(parts_in),
            out_specs=(sheet, piece),
            scratch_shapes=[pltpu.VMEM((sp, rows, per), bf16)],
            name="project",
        )(source, order, *mixed, *parts_in)
        projected, squares = pl.pallas_call(
            finish_kernel,
            grid=(out_cols // tile,),
            out_shape=(
                jax.ShapeDtypeStruct((rows, out_cols), bf16),
                jax.ShapeDtypeStruct((1, rows), f32),
            ),
            in_specs=[piece, slab, slab, sheet],
            out_specs=(sheet, pl.BlockSpec((1, rows), lambda n: (0, 0))),
            scratch_shapes=[pltpu.VMEM((rows, 128), f32)],
            name="finish",
        )(far_piece, *far, partial)
    squares = lax.psum(squares[0], "tp")
    scale = lax.rsqrt(squares / width + epsilon)
    gain = lax.dynamic_slice_in_dim(branch_norm_gain, tp_at * out_cols, out_cols)
    branch = projected.astype(f32) * scale[:, None] * gain
    return (residual.astype(f32) + branch).astype(bf16)


def solution(mesh):
    placed = (
        P("sp", "tp"),
        P("sp", "tp"),
        P("sp", "tp"),
        P("sp", "tp"),
        P(),
        P("tp", "sp"),
        P(),
        P("sp", "tp"),
        P(),
        P("sp", "tp"),
    )
    return jax.shard_map(
        per_device, mesh=mesh, in_specs=placed, out_specs=P("sp", "tp"), check_vma=False
    )
```

```python
import functools

import jax
import jax.numpy as jnp
from jax import lax
from jax.experimental import pallas as pl
from jax.experimental.pallas import tpu as pltpu
from jax.sharding import PartitionSpec as P


HEAD_DIM = 128
SPAN = 128
EXTRA = 8
TILE = 256
epsilon = 1e-06


f32 = jnp.float32
bf16 = jnp.bfloat16
NN = (((1,), (0,)), ((), ()))
TN = (((0,), (0,)), ((), ()))
NT = (((1,), (1,)), ((), ()))


def dot(a, b, dims=NN):
    return lax.dot_general(a, b, dims, preferred_element_type=f32)


def split2(value):
    high = value.astype(bf16)
    return high, (value - high.astype(f32)).astype(bf16)


def input_gate(forget_logits, gap):
    return gap / (1.0 + jnp.exp(forget_logits.astype(f32)))


def pack_decay(decay):
    first, _ = split2(decay)
    second, third = split2(decay - first.astype(f32))
    rows = [t.astype(f32) for t in (first, second, third)]
    row = lax.broadcasted_iota(jnp.int32, (EXTRA, decay.shape[-1]), 0)
    out = jnp.where(row == 2, rows[2], 0.0)
    return jnp.where(row == 0, rows[0], jnp.where(row == 1, rows[1], out)).astype(bf16)


def unpack(ref, head):
    state = ref[head, :HEAD_DIM, :].astype(f32)
    decay = jnp.sum(ref[head, HEAD_DIM:, :].astype(f32), axis=0, keepdims=True)
    return state, decay


def states_kernel(first_ref, tp_ref, forget_ref, value_ref, surge_ref, gap_ref, running_ref, packed_ref, column_ref):
    step = pl.program_id(0)
    per = packed_ref.shape[0]
    rows = forget_ref.shape[0]

    @pl.when(step == 0)
    def _():
        column_ref[...] = jnp.transpose(surge_ref[...])

    column = lax.broadcasted_iota(jnp.int32, (SPAN, 2 * SPAN), 1) % SPAN
    lower = (column <= lax.broadcasted_iota(jnp.int32, (SPAN, 2 * SPAN), 0)).astype(bf16)
    surges = column_ref[...]
    lane = lax.broadcasted_iota(jnp.int32, surges.shape, 1)
    for i in range(per):
        cols = slice(i * HEAD_DIM, (i + 1) * HEAD_DIM)
        head = (first_ref[0] + step) * per + i
        gates = input_gate(forget_ref[:, cols], gap_ref[i])
        surge = jnp.sum(jnp.where(lane == head, surges, 0.0), axis=1, keepdims=True)
        high, low = split2(jnp.log1p(-gates) + surge)
        after = jnp.zeros((1, HEAD_DIM), f32)
        keys = []
        for start in reversed(range(0, rows, SPAN)):
            part = slice(start, start + SPAN)
            running = dot(lower, jnp.concatenate([high[part], low[part]], axis=0))
            running_ref[part, cols] = running
            after = after + running[SPAN - 1 :, :]
            keys.append((gates[part] * jnp.exp(after - running)).astype(bf16))
        keys = jnp.concatenate(keys[::-1], axis=0)
        packed_ref[i, :HEAD_DIM, :] = dot(value_ref[:, cols], keys, TN).astype(bf16)
        packed_ref[i, HEAD_DIM:, :] = pack_decay(jnp.exp(after))


def local_kernel(first_ref, tp_ref, query_ref, forget_ref, value_ref, running_ref, gap_ref, local_ref, reach_ref):
    rows = query_ref.shape[0]
    row = lax.broadcasted_iota(jnp.int32, (SPAN, SPAN), 0)
    causal = lax.broadcasted_iota(jnp.int32, (SPAN, SPAN), 1) <= row
    for i in range(query_ref.shape[1] // HEAD_DIM):
        cols = slice(i * HEAD_DIM, (i + 1) * HEAD_DIM)
        before = jnp.zeros((1, HEAD_DIM), f32)
        state = None
        for start in range(0, rows, SPAN):
            part = slice(start, start + SPAN)
            logits = query_ref[part, cols].astype(f32)
            queries = logits / (1.0 + jnp.exp(-logits)) * HEAD_DIM**-0.5
            gates = input_gate(forget_ref[part, cols], gap_ref[i])
            values = value_ref[part, cols]
            running = running_ref[part, cols]
            anchor = running[SPAN // 2 - 1 : SPAN // 2, :]
            total = running[SPAN - 1 :, :]
            late = (queries * jnp.exp(running - anchor)).astype(bf16)
            early = (gates * jnp.exp(anchor - running)).astype(bf16)
            scores = jnp.where(causal, dot(late, early, NT), 0.0).astype(bf16)
            out = dot(scores, values)
            faded = queries * jnp.exp(running)
            if state is not None:
                out = out + dot(faded.astype(bf16), state.astype(bf16), NT)
            local_ref[part, cols] = out
            reach_ref[part, cols] = (faded * jnp.exp(before)).astype(bf16)
            if start + SPAN < rows:
                keys = (gates * jnp.exp(total - running)).astype(bf16)
                fresh = dot(values, keys, TN)
                state = fresh if state is None else state * jnp.exp(total) + fresh
                before = before + total


def pair_kernel(odd_ref, own_ref, other_ref, out_ref):
    even = odd_ref[0] == 0
    for head in range(own_ref.shape[0]):
        own, own_decay = unpack(own_ref, head)
        other, other_decay = unpack(other_ref, head)
        mine = jnp.where(even, other_decay, 1.0)
        theirs = jnp.where(even, 1.0, own_decay)
        out_ref[head, :HEAD_DIM, :] = (own * mine + other * theirs).astype(bf16)
        out_ref[head, HEAD_DIM:, :] = pack_decay(own_decay * other_decay)


def combine_kernel(earlier_ref, later_ref, out_ref):
    for head in range(later_ref.shape[0]):
        early, early_decay = unpack(earlier_ref, head)
        late, late_decay = unpack(later_ref, head)
        out_ref[head, :HEAD_DIM, :] = (early * late_decay + late).astype(bf16)
        out_ref[head, HEAD_DIM:, :] = pack_decay(early_decay * late_decay)


def carry_kernel(odd_ref, earlier_ref, later_ref, own_ref, other_ref, mine_ref, theirs_ref):
    odd = odd_ref[0] == 1
    for head in range(own_ref.shape[0]):
        early, _ = unpack(earlier_ref, head)
        late, late_decay = unpack(later_ref, head)
        before = early * late_decay + late
        own, own_decay = unpack(own_ref, head)
        other, other_decay = unpack(other_ref, head)
        first = jnp.where(odd, other, own)
        decay = jnp.where(odd, other_decay, own_decay)
        after = before * decay + first
        mine_ref[head] = jnp.where(odd, after, before).astype(bf16)
        theirs_ref[head] = jnp.where(odd, before, after).astype(bf16)


def mix_kernel(first_ref, local_ref, reach_ref, carried_ref, gate_ref, gain_ref, out_ref):
    for i in range(carried_ref.shape[0]):
        cols = slice(i * HEAD_DIM, (i + 1) * HEAD_DIM)
        heads_out = local_ref[:, cols] + dot(reach_ref[:, cols], carried_ref[i], NT)
        mean_sq = jnp.mean(heads_out * heads_out, axis=1, keepdims=True)
        logits = gate_ref[:, cols].astype(f32)
        gates = logits / (1.0 + jnp.exp(-logits))
        mixed = heads_out * lax.rsqrt(mean_sq + epsilon) * gain_ref[...] * gates
        out_ref[:, cols] = mixed.astype(bf16)


def ring_at(place, size):
    return jnp.where(place < size // 2, 2 * place, 2 * (size - 1 - place) + 1)


def place_of(member, size):
    return jnp.where(member % 2 == 0, member // 2, size - 1 - member // 2)


def near_kernel(sp_ref, tp_ref, *refs, offsets, size, n_mixed):
    mixed = refs[:n_mixed]
    chunks = refs[n_mixed:-2]
    out_ref, table = refs[-2:]
    at = place_of(sp_ref[0], size)
    per = 2

    @pl.when(pl.program_id(0) == 0)
    def _():
        for i, piece in enumerate(mixed):
            group = (i + sp_ref[0]) % 2
            table[(tp_ref[0] ^ (i // per)) * per + group] = piece[...]

    total = None
    half = chunks[0].shape[0]
    for i, offset in enumerate(offsets):
        block = ring_at((at + (offset + size)) % size, size)
        for j in range(2):
            part = dot(table[block, :, j * half : (j + 1) * half], chunks[2 * i + j][...])
            total = part if total is None else total + part
    out_ref[...] = total


def far_kernel(sp_ref, *refs, offsets, size):
    table, partial_ref = refs[:2]
    chunks = refs[2:-1]
    out_ref = refs[-1]
    at = place_of(sp_ref[0], size)
    total = partial_ref[...]
    half = chunks[0].shape[0]
    for i, offset in enumerate(offsets):
        block = ring_at((at + (offset + size)) % size, size)
        for j in range(2):
            total = total + dot(table[block, :, j * half : (j + 1) * half], chunks[2 * i + j][...])
    out_ref[...] = total


def last_kernel(sp_ref, table, partial_ref, first_ref, second_ref, out_ref, square_ref, lanes_ref, *, size):
    del sp_ref
    half = first_ref.shape[0]
    total = partial_ref[...] + dot(table[0, :, :half], first_ref[...])
    total = total + dot(table[0, :, half:], second_ref[...])
    rounded = total.astype(bf16)
    out_ref[...] = rounded
    wide = rounded.astype(f32)
    squares = wide * wide
    lanes = squares[:, :128]
    for start in range(128, squares.shape[1], 128):
        lanes = lanes + squares[:, start : start + 128]

    @pl.when(pl.program_id(0) == 0)
    def _():
        lanes_ref[...] = lanes

    @pl.when(pl.program_id(0) > 0)
    def _():
        lanes_ref[...] += lanes

    @pl.when(pl.program_id(0) == pl.num_programs(0) - 1)
    def _():
        high, low = split2(lanes_ref[...])
        ones = jnp.ones((8, 128), bf16)
        square_ref[...] = (dot(ones, high, NT) + dot(ones, low, NT))[:1]


def norm_kernel(tp_ref, square_ref, projected_ref, residual_ref, gain_ref, out_ref, *, width):
    squares = jnp.broadcast_to(square_ref[...], (8, square_ref.shape[1]))
    scale = lax.rsqrt(jnp.transpose(squares)[:, :1] / width + epsilon)
    branch = projected_ref[...].astype(f32) * scale * gain_ref[...]
    out_ref[...] = (residual_ref[...].astype(f32) + branch).astype(bf16)


def vmem():
    return pl.BlockSpec(memory_space=pltpu.VMEM)


def smem():
    return pl.BlockSpec(memory_space=pltpu.SMEM)


def call(kernel, scalars, operands, out_shape, grid, in_specs, out_specs, scratch=()):
    spec = pltpu.PrefetchScalarGridSpec(
        num_scalar_prefetch=len(scalars),
        grid=grid,
        in_specs=in_specs,
        out_specs=out_specs,
        scratch_shapes=list(scratch),
    )
    return pl.pallas_call(kernel, grid_spec=spec, out_shape=out_shape)(*scalars, *operands)


def permute(array, axis, pairs):
    return lax.ppermute(array, axis, pairs)


def is_ringed(sp, tp):
    return sp == 2 * tp and sp <= 8


def ring_gather(own, axis):
    size = lax.axis_size(axis)
    ring = list(range(0, size, 2)) + list(range(1, size, 2))[::-1]
    forward = [(ring[i], ring[(i + 1) % size]) for i in range(size)]
    backward = [(b, a) for a, b in forward]
    half = own.shape[0] // 2
    chunks = {0: (own[:half], own[half:])}
    for step in range(1, size // 2):
        chunks[-step], chunks[step] = [None, None], [None, None]
        for part in range(2):
            for sign, pairs in ((-1, forward), (1, backward)):
                chunks[sign * step][part] = permute(chunks[sign * (step - 1)][part], axis, pairs)
    last = size // 2
    chunks[last] = (permute(chunks[1 - last][0], axis, forward), permute(chunks[last - 1][1], axis, backward))
    return chunks


def swap(array, axis, bit):
    size = lax.axis_size(axis)
    return permute(array, axis, [(i, i ^ bit) for i in range(size)])


def shift(array, axis, by):
    size = lax.axis_size(axis)
    return permute(array, axis, [(i, i + by) for i in range(size - by)])


def carried_states(given, kept, axis, odd):
    size = lax.axis_size(axis)
    like = jax.ShapeDtypeStruct(kept.shape, kept.dtype)
    other = swap(given, axis, 1)
    pair = pl.pallas_call(pair_kernel, out_shape=like, in_specs=[smem(), vmem(), vmem()], out_specs=vmem(), name="pair")(odd, kept, other)

    def combine(earlier, later):
        return pl.pallas_call(combine_kernel, out_shape=like, in_specs=[vmem(), vmem()], out_specs=vmem(), name="combine")(earlier, later)

    earlier, later = shift(pair, axis, 2), None
    reach = 2
    while reach < size // 2:
        before = earlier if later is None else combine(earlier, later)
        earlier, later = shift(combine(before, pair), axis, 2 * reach), before
        reach *= 2
    state = jax.ShapeDtypeStruct((kept.shape[0], HEAD_DIM, HEAD_DIM), bf16)
    mine, theirs = pl.pallas_call(
        carry_kernel,
        out_shape=(state, state),
        in_specs=[smem()] + [vmem()] * 4,
        out_specs=(vmem(), vmem()),
        name="carry",
    )(odd, earlier, later, kept, other)
    return mine, swap(theirs, axis, 1)


def layer(
    query_logits,
    forget_logits,
    value_inputs,
    output_gate_logits,
    forget_floor_gap,
    surge_log_decay,
    head_norm_gain,
    output_matrix,
    branch_norm_gain,
    residual,
):
    rows, head_cols = query_logits.shape
    heads = head_cols // HEAD_DIM
    sp, tp = lax.axis_size("sp"), lax.axis_size("tp")
    sp_at = lax.axis_index("sp").astype(jnp.int32).reshape(1)
    tp_at = lax.axis_index("tp").astype(jnp.int32).reshape(1)
    odd = sp_at % 2
    width = output_matrix.shape[0] * sp
    out_cols = output_matrix.shape[1]
    ringed = is_ringed(sp, tp)

    if ringed:
        chunks = ring_gather(output_matrix, "sp")
    else:
        whole_weight = lax.all_gather(output_matrix, "sp", axis=0, tiled=True)

    group = heads // 2
    per = 2
    steps = group // per
    gap = forget_floor_gap.reshape(-1, 1, HEAD_DIM)
    block = pl.BlockSpec((rows, per * HEAD_DIM), lambda s, first, at: (0, first[0] + s))
    own_block = pl.BlockSpec((rows, per * HEAD_DIM), lambda s, first, at: (0, s))
    gap_block = pl.BlockSpec((per, 1, HEAD_DIM), lambda s, first, at: (at[0] * (heads // per) + first[0] + s, 0, 0))
    wide = jax.ShapeDtypeStruct((rows, group * HEAD_DIM), f32)
    narrow = jax.ShapeDtypeStruct((rows, group * HEAD_DIM), bf16)

    def group_states(first):
        return call(
            states_kernel,
            (first, tp_at),
            (forget_logits, value_inputs, surge_log_decay, gap),
            (wide, jax.ShapeDtypeStruct((group, HEAD_DIM + EXTRA, HEAD_DIM), bf16)),
            (steps,),
            [block, block, pl.BlockSpec((heads, rows), lambda s, first, at: (0, 0)), gap_block],
            (own_block, pl.BlockSpec((per, HEAD_DIM + EXTRA, HEAD_DIM), lambda s, first, at: (s, 0, 0))),
            [pltpu.VMEM((rows, heads), f32)],
        )

    def group_local(first, running):
        return call(
            local_kernel,
            (first, tp_at),
            (query_logits, forget_logits, value_inputs, running, gap),
            (wide, narrow),
            (steps,),
            [block, block, block, own_block, gap_block],
            (own_block, own_block),
        )

    def group_mix(first, local, reach, carried):
        shared = pl.BlockSpec((rows, per * HEAD_DIM), lambda s, first: (0, s))
        return call(
            mix_kernel,
            (first,),
            (local, reach, carried, output_gate_logits, head_norm_gain.reshape(1, HEAD_DIM)),
            narrow,
            (steps,),
            [
                shared,
                shared,
                pl.BlockSpec((per, HEAD_DIM, HEAD_DIM), lambda s, first: (s, 0, 0)),
                pl.BlockSpec((rows, per * HEAD_DIM), lambda s, first: (0, first[0] + s)),
                pl.BlockSpec((1, HEAD_DIM), lambda s, first: (0, 0)),
            ],
            shared,
        )

    given_first, kept_first = (1 - odd) * steps, odd * steps
    given_running, given = group_states(given_first)
    kept_running, kept = group_states(kept_first)
    mine, others = carried_states(given, kept, "sp", odd)
    kept_local = group_local(kept_first, kept_running)
    given_local = group_local(given_first, given_running)
    pieces = {0: [group_mix(kept_first, *kept_local, mine), group_mix(given_first, *given_local, others)]}
    bit = tp // 2
    while bit:
        for rel in sorted(pieces):
            pieces[rel ^ bit] = [swap(piece, "tp", bit) for piece in pieces[rel]]
        bit //= 2
    mixed = [piece for rel in range(tp) for piece in pieces[rel]]

    tile = min(TILE, out_cols)
    grid = (out_cols // tile,)
    if ringed:
        last = sp // 2
        cols = group * HEAD_DIM
        chunk = cols // 2
        partial_sum = jax.ShapeDtypeStruct((rows, out_cols), f32)
        piece_spec = lambda: pl.BlockSpec((rows, cols), lambda n, *_: (0, 0))
        slab = pl.BlockSpec((chunk, tile), lambda n, *_: (0, n))
        sheet = pl.BlockSpec((rows, tile), lambda n, *_: (0, n))
        whole_table = pl.BlockSpec((sp, rows, cols), lambda n, *_: (0, 0, 0))
        near = [0] + [s * k for k in range(1, last - 1) for s in (-1, 1)]
        far = [s * (last - 1) for s in (-1, 1)]
        partial, table = call(
            functools.partial(near_kernel, offsets=near, size=sp, n_mixed=len(mixed)),
            (sp_at, tp_at),
            (*mixed, *[half for off in near for half in chunks[off]]),
            (partial_sum, jax.ShapeDtypeStruct((sp, rows, cols), bf16)),
            grid,
            [piece_spec()] * len(mixed) + [slab] * (2 * len(near)),
            (sheet, whole_table),
        )
        partial = call(
            functools.partial(far_kernel, offsets=far, size=sp),
            (sp_at,),
            (table, partial, *[half for off in far for half in chunks[off]]),
            partial_sum,
            grid,
            [whole_table, sheet] + [slab] * (2 * len(far)),
            sheet,
        )
        projected, squares = call(
            functools.partial(last_kernel, size=sp),
            (sp_at,),
            (table, partial, *chunks[last]),
            (jax.ShapeDtypeStruct((rows, out_cols), bf16), jax.ShapeDtypeStruct((1, rows), f32)),
            grid,
            [
                pl.BlockSpec((1, rows, cols), lambda n, at: (ring_at((place_of(at[0], sp) + last) % sp, sp), 0, 0)),
                sheet,
                slab,
                slab,
            ],
            (sheet, pl.BlockSpec((1, rows), lambda n, at: (0, 0))),
            [pltpu.VMEM((rows, 128), f32)],
        )
    else:
        stacked = jnp.stack(mixed)
        index = jnp.arange(2 * tp, dtype=jnp.int32)
        where = ((index // 2) ^ tp_at[0]) * 2 + (index + odd[0]) % 2
        all_heads = jnp.moveaxis(stacked[where], 0, 1).reshape(rows, width)
        projected = jnp.dot(all_heads, whole_weight, preferred_element_type=f32).astype(bf16)
        branch = lax.optimization_barrier(projected).astype(f32)
        squares = jnp.sum(branch * branch, axis=1)[None]
    squares = lax.psum(squares, "tp")
    sheet = pl.BlockSpec((rows, tile), lambda n, at: (0, n))
    return call(
        functools.partial(norm_kernel, width=width),
        (tp_at,),
        (squares, projected, residual, branch_norm_gain.reshape(1, -1)),
        jax.ShapeDtypeStruct((rows, out_cols), bf16),
        grid,
        [
            pl.BlockSpec((1, rows), lambda n, at: (0, 0)),
            sheet,
            sheet,
            pl.BlockSpec((1, tile), lambda n, at: (0, at[0] * (out_cols // tile) + n)),
        ],
        sheet,
    )


def solution(mesh):
    placed = (
        P("sp", "tp"),
        P("sp", "tp"),
        P("sp", "tp"),
        P("sp", "tp"),
        P(),
        P("tp", "sp"),
        P(),
        P("sp", "tp"),
        P(),
        P("sp", "tp"),
    )
    return jax.shard_map(layer, mesh=mesh, in_specs=placed, out_specs=P("sp", "tp"), check_vma=False)
```

```python
import functools

import jax
import jax.numpy as jnp
from jax import lax
from jax.experimental import pallas as pl
from jax.experimental.pallas import tpu as pltpu
from jax.sharding import PartitionSpec as P


HEAD_DIM = 128
SPAN = 128
EXTRA = 8
TILE = 256
ROOM = pltpu.CompilerParams(vmem_limit_bytes=32 * 2**20)
epsilon = 1e-06


f32 = jnp.float32
bf16 = jnp.bfloat16
NN = (((1,), (0,)), ((), ()))
TN = (((0,), (0,)), ((), ()))
NT = (((1,), (1,)), ((), ()))


def dot(a, b, dims=NN):
    return lax.dot_general(a, b, dims, preferred_element_type=f32)


def split2(value):
    high = value.astype(bf16)
    return high, (value - high.astype(f32)).astype(bf16)


def input_gate(forget_logits, gap):
    return gap / (1.0 + jnp.exp(forget_logits.astype(f32)))


def pack_decay(decay):
    first, _ = split2(decay)
    second, third = split2(decay - first.astype(f32))
    rows = [t.astype(f32) for t in (first, second, third)]
    row = lax.broadcasted_iota(jnp.int32, (EXTRA, decay.shape[-1]), 0)
    out = jnp.where(row == 2, rows[2], 0.0)
    return jnp.where(row == 0, rows[0], jnp.where(row == 1, rows[1], out)).astype(bf16)


def unpack(ref, head):
    state = ref[head, :HEAD_DIM, :].astype(f32)
    decay = jnp.sum(ref[head, HEAD_DIM:, :].astype(f32), axis=0, keepdims=True)
    return state, decay


def states_kernel(first_ref, tp_ref, forget_ref, value_ref, surge_ref, gap_ref, running_ref, packed_ref, column_ref):
    step = pl.program_id(0)
    per = gap_ref.shape[0]
    rows = forget_ref.shape[0]

    @pl.when(step == 0)
    def _():
        column_ref[...] = jnp.transpose(surge_ref[...])

    column = lax.broadcasted_iota(jnp.int32, (SPAN, 2 * SPAN), 1) % SPAN
    lower = (column <= lax.broadcasted_iota(jnp.int32, (SPAN, 2 * SPAN), 0)).astype(bf16)
    surges = column_ref[...]
    lane = lax.broadcasted_iota(jnp.int32, surges.shape, 1)
    for i in range(per):
        cols = slice(i * HEAD_DIM, (i + 1) * HEAD_DIM)
        head = (first_ref[0] + step) * per + i
        gates = input_gate(forget_ref[:, cols], gap_ref[i])
        surge = jnp.sum(jnp.where(lane == head, surges, 0.0), axis=1, keepdims=True)
        high, low = split2(jnp.log1p(-gates) + surge)
        after = jnp.zeros((1, HEAD_DIM), f32)
        keys = []
        for start in reversed(range(0, rows, SPAN)):
            part = slice(start, start + SPAN)
            running = dot(lower, jnp.concatenate([high[part], low[part]], axis=0))
            running_ref[part, cols] = running
            after = after + running[SPAN - 1 :, :]
            keys.append((gates[part] * jnp.exp(after - running)).astype(bf16))
        keys = jnp.concatenate(keys[::-1], axis=0)
        packed_ref[step * per + i, :HEAD_DIM, :] = dot(value_ref[:, cols], keys, TN).astype(bf16)
        packed_ref[step * per + i, HEAD_DIM:, :] = pack_decay(jnp.exp(after))


def local_kernel(first_ref, tp_ref, query_ref, forget_ref, value_ref, running_ref, gap_ref, local_ref, reach_ref):
    rows = query_ref.shape[0]
    row = lax.broadcasted_iota(jnp.int32, (SPAN, SPAN), 0)
    causal = lax.broadcasted_iota(jnp.int32, (SPAN, SPAN), 1) <= row
    for i in range(query_ref.shape[1] // HEAD_DIM):
        cols = slice(i * HEAD_DIM, (i + 1) * HEAD_DIM)
        before = jnp.zeros((1, HEAD_DIM), f32)
        state = None
        for start in range(0, rows, SPAN):
            part = slice(start, start + SPAN)
            logits = query_ref[part, cols].astype(f32)
            queries = logits / (1.0 + jnp.exp(-logits)) * HEAD_DIM**-0.5
            gates = input_gate(forget_ref[part, cols], gap_ref[i])
            values = value_ref[part, cols]
            running = running_ref[part, cols]
            anchor = running[SPAN // 2 - 1 : SPAN // 2, :]
            total = running[SPAN - 1 :, :]
            late = (queries * jnp.exp(running - anchor)).astype(bf16)
            early = (gates * jnp.exp(anchor - running)).astype(bf16)
            scores = jnp.where(causal, dot(late, early, NT), 0.0).astype(bf16)
            out = dot(scores, values)
            faded = queries * jnp.exp(running)
            if state is not None:
                out = out + dot(faded.astype(bf16), state.astype(bf16), NT)
            local_ref[part, cols] = out
            reach_ref[part, cols] = (faded * jnp.exp(before)).astype(bf16)
            if start + SPAN < rows:
                keys = (gates * jnp.exp(total - running)).astype(bf16)
                fresh = dot(values, keys, TN)
                state = fresh if state is None else state * jnp.exp(total) + fresh
                before = before + total


def pair_kernel(odd_ref, own_ref, other_ref, out_ref):
    even = odd_ref[0] == 0
    for head in range(own_ref.shape[0]):
        own, own_decay = unpack(own_ref, head)
        other, other_decay = unpack(other_ref, head)
        mine = jnp.where(even, other_decay, 1.0)
        theirs = jnp.where(even, 1.0, own_decay)
        out_ref[head, :HEAD_DIM, :] = (own * mine + other * theirs).astype(bf16)
        out_ref[head, HEAD_DIM:, :] = pack_decay(own_decay * other_decay)


def combine_kernel(earlier_ref, later_ref, out_ref):
    for head in range(later_ref.shape[0]):
        early, early_decay = unpack(earlier_ref, head)
        late, late_decay = unpack(later_ref, head)
        out_ref[head, :HEAD_DIM, :] = (early * late_decay + late).astype(bf16)
        out_ref[head, HEAD_DIM:, :] = pack_decay(early_decay * late_decay)


def carry_kernel(odd_ref, earlier_ref, later_ref, own_ref, other_ref, mine_ref, theirs_ref):
    odd = odd_ref[0] == 1
    for head in range(own_ref.shape[0]):
        early, _ = unpack(earlier_ref, head)
        late, late_decay = unpack(later_ref, head)
        before = early * late_decay + late
        own, own_decay = unpack(own_ref, head)
        other, other_decay = unpack(other_ref, head)
        first = jnp.where(odd, other, own)
        decay = jnp.where(odd, other_decay, own_decay)
        after = before * decay + first
        mine_ref[head] = jnp.where(odd, after, before).astype(bf16)
        theirs_ref[head] = jnp.where(odd, before, after).astype(bf16)


def mix_kernel(first_ref, local_ref, reach_ref, carried_ref, gate_ref, gain_ref, out_ref):
    per = out_ref.shape[1] // HEAD_DIM
    for i in range(per):
        cols = slice(i * HEAD_DIM, (i + 1) * HEAD_DIM)
        carried = carried_ref[pl.program_id(0) * per + i]
        heads_out = local_ref[:, cols] + dot(reach_ref[:, cols], carried, NT)
        mean_sq = jnp.mean(heads_out * heads_out, axis=1, keepdims=True)
        logits = gate_ref[:, cols].astype(f32)
        gates = logits / (1.0 + jnp.exp(-logits))
        mixed = heads_out * lax.rsqrt(mean_sq + epsilon) * gain_ref[...] * gates
        out_ref[:, cols] = mixed.astype(bf16)


def ring_at(place, size):
    return jnp.where(place < size // 2, 2 * place, 2 * (size - 1 - place) + 1)


def place_of(member, size):
    return jnp.where(member % 2 == 0, member // 2, size - 1 - member // 2)


def project_kernel(sp_ref, tp_ref, *refs, offsets, size, n_mixed):
    mixed = refs[:n_mixed]
    chunks = refs[n_mixed:-3]
    out_ref, piece_ref, table = refs[-3:]
    at = place_of(sp_ref[0], size)
    half = chunks[0].shape[0]
    for i, piece in enumerate(mixed):
        group = (i + sp_ref[0]) % 2
        table[(tp_ref[0] ^ (i // 2)) * 2 + group] = piece[...]
    piece_ref[...] = table[ring_at((at + size // 2) % size, size)]
    for start in range(0, out_ref.shape[1], TILE):
        cols = slice(start, start + TILE)
        total = None
        for i, offset in enumerate(offsets):
            block = ring_at((at + (offset + size)) % size, size)
            for j in range(2):
                part = dot(table[block, :, j * half : (j + 1) * half], chunks[2 * i + j][:, cols])
                total = part if total is None else total + part
        out_ref[:, cols] = total


def last_kernel(partial_ref, piece_ref, first_ref, second_ref, out_ref, square_ref, lanes_ref):
    half = first_ref.shape[0]
    for start in range(0, out_ref.shape[1], TILE):
        cols = slice(start, start + TILE)
        total = partial_ref[:, cols] + dot(piece_ref[:, :half], first_ref[:, cols])
        rounded = (total + dot(piece_ref[:, half:], second_ref[:, cols])).astype(bf16)
        out_ref[:, cols] = rounded
        wide = rounded.astype(f32)
        squares = wide * wide
        lanes = squares[:, :128]
        for first in range(128, TILE, 128):
            lanes = lanes + squares[:, first : first + 128]
        lanes_ref[...] = lanes if start == 0 else lanes_ref[...] + lanes
    high, low = split2(lanes_ref[...])
    ones = jnp.ones((8, 128), bf16)
    square_ref[...] = (dot(ones, high, NT) + dot(ones, low, NT))[:1]


def norm_kernel(tp_ref, square_ref, projected_ref, residual_ref, gain_ref, out_ref, *, width):
    squares = jnp.broadcast_to(square_ref[...], (8, square_ref.shape[1]))
    scale = lax.rsqrt(jnp.transpose(squares)[:, :1] / width + epsilon)
    branch = projected_ref[...].astype(f32) * scale * gain_ref[...]
    out_ref[...] = (residual_ref[...].astype(f32) + branch).astype(bf16)


def vmem():
    return pl.BlockSpec(memory_space=pltpu.VMEM)


def smem():
    return pl.BlockSpec(memory_space=pltpu.SMEM)


def resident(array):
    return pltpu.with_memory_space_constraint(array, pltpu.VMEM)


def small(kernel, scalars, operands, outs, scratch=()):
    return pl.pallas_call(
        kernel,
        out_shape=tuple(pltpu.VMEM(*out) for out in outs),
        in_specs=[smem()] * len(scalars) + [vmem()] * len(operands),
        out_specs=tuple(vmem() for _ in outs),
        scratch_shapes=list(scratch),
        compiler_params=ROOM,
    )(*scalars, *[resident(array) for array in operands])


def call(kernel, scalars, operands, out_shape, grid, in_specs, out_specs, scratch=()):
    spec = pltpu.PrefetchScalarGridSpec(
        num_scalar_prefetch=len(scalars),
        grid=grid,
        in_specs=in_specs,
        out_specs=out_specs,
        scratch_shapes=list(scratch),
    )
    return pl.pallas_call(kernel, grid_spec=spec, out_shape=out_shape, compiler_params=ROOM)(*scalars, *operands)


def permute(array, axis, pairs):
    return lax.ppermute(array, axis, pairs)


def is_ringed(sp, tp):
    return sp == 2 * tp and sp <= 8


def ring_gather(own, axis):
    size = lax.axis_size(axis)
    ring = list(range(0, size, 2)) + list(range(1, size, 2))[::-1]
    forward = [(ring[i], ring[(i + 1) % size]) for i in range(size)]
    backward = [(b, a) for a, b in forward]
    half = own.shape[0] // 2
    chunks = {0: (own[:half], own[half:])}
    for step in range(1, size // 2):
        chunks[-step], chunks[step] = [None, None], [None, None]
        for part in range(2):
            for sign, pairs in ((-1, forward), (1, backward)):
                chunks[sign * step][part] = permute(chunks[sign * (step - 1)][part], axis, pairs)
    last = size // 2
    chunks[last] = (
        permute(chunks[1 - last][0], axis, forward), permute(chunks[last - 1][1], axis, backward)
    )
    return chunks


def swap(array, axis, bit):
    size = lax.axis_size(axis)
    return permute(array, axis, [(i, i ^ bit) for i in range(size)])


def shift(array, axis, by):
    size = lax.axis_size(axis)
    return permute(array, axis, [(i, i + by) for i in range(size - by)])


def carried_states(given, kept, axis, odd):
    size = lax.axis_size(axis)
    other = swap(given, axis, 1)
    (pair,) = small(pair_kernel, (odd,), (kept, other), [(kept.shape, bf16)])

    def combine(earlier, later):
        return small(combine_kernel, (), (earlier, later), [(later.shape, bf16)])[0]

    earlier, later = shift(pair, axis, 2), None
    reach = 2
    while reach < size // 2:
        before = earlier if later is None else combine(earlier, later)
        earlier, later = shift(combine(before, pair), axis, 2 * reach), before
        reach *= 2
    state = ((kept.shape[0], HEAD_DIM, HEAD_DIM), bf16)
    mine, theirs = small(carry_kernel, (odd,), (earlier, later, kept, other), [state, state])
    return mine, swap(theirs, axis, 1)


def layer(
    query_logits,
    forget_logits,
    value_inputs,
    output_gate_logits,
    forget_floor_gap,
    surge_log_decay,
    head_norm_gain,
    output_matrix,
    branch_norm_gain,
    residual,
):
    rows, head_cols = query_logits.shape
    heads = head_cols // HEAD_DIM
    sp, tp = lax.axis_size("sp"), lax.axis_size("tp")
    sp_at = lax.axis_index("sp").astype(jnp.int32).reshape(1)
    tp_at = lax.axis_index("tp").astype(jnp.int32).reshape(1)
    odd = sp_at % 2
    width = output_matrix.shape[0] * sp
    out_cols = output_matrix.shape[1]
    ringed = is_ringed(sp, tp)

    if ringed:
        chunks = ring_gather(output_matrix, "sp")
    else:
        whole_weight = lax.all_gather(output_matrix, "sp", axis=0, tiled=True)

    group = heads // 2
    per = 2
    steps = group // per
    gap = forget_floor_gap.reshape(-1, 1, HEAD_DIM)
    block = pl.BlockSpec((rows, per * HEAD_DIM), lambda s, first, at: (0, first[0] + s))
    own_block = pl.BlockSpec((rows, per * HEAD_DIM), lambda s, first, at: (0, s))
    gap_block = pl.BlockSpec((per, 1, HEAD_DIM), lambda s, first, at: (at[0] * (heads // per) + first[0] + s, 0, 0))
    wide = jax.ShapeDtypeStruct((rows, group * HEAD_DIM), f32)
    narrow = jax.ShapeDtypeStruct((rows, group * HEAD_DIM), bf16)

    def group_states(first):
        return call(
            states_kernel,
            (first, tp_at),
            (forget_logits, value_inputs, surge_log_decay, gap),
            (wide, pltpu.VMEM((group, HEAD_DIM + EXTRA, HEAD_DIM), bf16)),
            (steps,),
            [block, block, pl.BlockSpec((heads, rows), lambda s, first, at: (0, 0)), gap_block],
            (own_block, vmem()),
            [pltpu.VMEM((rows, heads), f32)],
        )

    def group_local(first, running):
        return call(
            local_kernel,
            (first, tp_at),
            (query_logits, forget_logits, value_inputs, running, gap),
            (wide, narrow),
            (steps,),
            [block, block, block, own_block, gap_block],
            (own_block, own_block),
        )

    def group_mix(first, local, reach, carried):
        shared = pl.BlockSpec((rows, per * HEAD_DIM), lambda s, first: (0, s))
        return call(
            mix_kernel,
            (first,),
            (local, reach, resident(carried), output_gate_logits, head_norm_gain.reshape(1, HEAD_DIM)),
            narrow,
            (steps,),
            [
                shared,
                shared,
                vmem(),
                pl.BlockSpec((rows, per * HEAD_DIM), lambda s, first: (0, first[0] + s)),
                pl.BlockSpec((1, HEAD_DIM), lambda s, first: (0, 0)),
            ],
            shared,
        )

    given_first, kept_first = (1 - odd) * steps, odd * steps
    given_running, given = group_states(given_first)
    kept_running, kept = group_states(kept_first)
    mine, others = carried_states(given, kept, "sp", odd)
    kept_local = group_local(kept_first, kept_running)
    given_local = group_local(given_first, given_running)
    pieces = {
        0: [group_mix(kept_first, *kept_local, mine), group_mix(given_first, *given_local, others)]
    }
    bit = tp // 2
    while bit:
        for rel in sorted(pieces):
            pieces[rel ^ bit] = [swap(piece, "tp", bit) for piece in pieces[rel]]
        bit //= 2
    mixed = [piece for rel in range(tp) for piece in pieces[rel]]

    if ringed:
        offsets = [0] + [s * k for k in range(1, sp // 2) for s in (-1, 1)]
        operands = [*mixed, *[half for off in offsets for half in chunks[off]]]
        columns = group * HEAD_DIM
        partial, piece = small(
            functools.partial(project_kernel, offsets=offsets, size=sp, n_mixed=len(mixed)),
            (sp_at, tp_at),
            operands,
            [((rows, out_cols), f32), ((rows, columns), bf16)],
            [pltpu.VMEM((sp, rows, columns), bf16)],
        )
        projected, squares = small(
            last_kernel,
            (),
            (partial, piece, *chunks[sp // 2]),
            [((rows, out_cols), bf16), ((1, rows), f32)],
            [pltpu.VMEM((rows, 128), f32)],
        )
    else:
        stacked = jnp.stack(mixed)
        index = jnp.arange(2 * tp, dtype=jnp.int32)
        where = ((index // 2) ^ tp_at[0]) * 2 + (index + odd[0]) % 2
        all_heads = jnp.moveaxis(stacked[where], 0, 1).reshape(rows, width)
        projected = jnp.dot(all_heads, whole_weight, preferred_element_type=f32).astype(bf16)
        branch = lax.optimization_barrier(projected).astype(f32)
        squares = jnp.sum(branch * branch, axis=1)[None]
    squares = lax.psum(squares, "tp")
    tile = rows // 4
    sheet = pl.BlockSpec((tile, out_cols), lambda n, at: (n, 0))
    return call(
        functools.partial(norm_kernel, width=width),
        (tp_at,),
        (squares, projected, residual, branch_norm_gain.reshape(1, -1)),
        jax.ShapeDtypeStruct((rows, out_cols), bf16),
        (rows // tile,),
        [
            pl.BlockSpec((1, tile), lambda n, at: (0, n)),
            sheet,
            sheet,
            pl.BlockSpec((1, out_cols), lambda n, at: (0, at[0])),
        ],
        sheet,
    )


def solution(mesh):
    placed = (
        P("sp", "tp"),
        P("sp", "tp"),
        P("sp", "tp"),
        P("sp", "tp"),
        P(),
        P("tp", "sp"),
        P(),
        P("sp", "tp"),
        P(),
        P("sp", "tp"),
    )
    return jax.shard_map(
        layer, mesh=mesh, in_specs=placed, out_specs=P("sp", "tp"), check_vma=False
    )
```

```python
import functools

import jax
import jax.numpy as jnp
from jax import lax
from jax.experimental import pallas as pl
from jax.experimental.pallas import tpu as pltpu
from jax.sharding import PartitionSpec as P


HEAD_DIM = 128
SPAN = 128
EXTRA = 8
TILE = 256
ROOM = pltpu.CompilerParams(vmem_limit_bytes=32 * 2**20)
epsilon = 1e-06


f32 = jnp.float32
bf16 = jnp.bfloat16
NN = (((1,), (0,)), ((), ()))
TN = (((0,), (0,)), ((), ()))
NT = (((1,), (1,)), ((), ()))


def dot(a, b, dims=NN):
    return lax.dot_general(a, b, dims, preferred_element_type=f32)


def split2(value):
    high = value.astype(bf16)
    return high, (value - high.astype(f32)).astype(bf16)


def input_gate(forget_logits, gap):
    return gap / (1.0 + jnp.exp(forget_logits.astype(f32)))


def pack_decay(decay):
    first, _ = split2(decay)
    second, third = split2(decay - first.astype(f32))
    rows = [t.astype(f32) for t in (first, second, third)]
    row = lax.broadcasted_iota(jnp.int32, (EXTRA, decay.shape[-1]), 0)
    out = jnp.where(row == 2, rows[2], 0.0)
    return jnp.where(row == 0, rows[0], jnp.where(row == 1, rows[1], out)).astype(bf16)


def unpack(ref, head):
    state = ref[head, :HEAD_DIM, :].astype(f32)
    decay = jnp.sum(ref[head, HEAD_DIM:, :].astype(f32), axis=0, keepdims=True)
    return state, decay


def halves_kernel(matrix_ref, *refs):
    halves, sems = refs[:-1], refs[-1]
    rows = halves[0].shape[0]
    copies = []
    for i, half_ref in enumerate(halves):
        copies.append(pltpu.make_async_copy(matrix_ref.at[pl.ds(i * rows, rows)], half_ref, sems.at[i]))
        copies[-1].start()
    for copy in copies:
        copy.wait()


def states_kernel(first_ref, tp_ref, forget_ref, value_ref, surge_ref, gap_ref, running_ref, packed_ref, column_ref):
    step = pl.program_id(0)
    per = gap_ref.shape[0]
    rows = forget_ref.shape[0]

    @pl.when(step == 0)
    def _():
        column_ref[...] = jnp.transpose(surge_ref[...])

    column = lax.broadcasted_iota(jnp.int32, (SPAN, 2 * SPAN), 1) % SPAN
    lower = (column <= lax.broadcasted_iota(jnp.int32, (SPAN, 2 * SPAN), 0)).astype(bf16)
    surges = column_ref[...]
    lane = lax.broadcasted_iota(jnp.int32, surges.shape, 1)
    for i in range(per):
        cols = slice(i * HEAD_DIM, (i + 1) * HEAD_DIM)
        head = (first_ref[0] + step) * per + i
        gates = input_gate(forget_ref[:, cols], gap_ref[i])
        surge = jnp.sum(jnp.where(lane == head, surges, 0.0), axis=1, keepdims=True)
        high, low = split2(jnp.log1p(-gates) + surge)
        after = jnp.zeros((1, HEAD_DIM), f32)
        keys = []
        for start in reversed(range(0, rows, SPAN)):
            part = slice(start, start + SPAN)
            running = dot(lower, jnp.concatenate([high[part], low[part]], axis=0))
            running_ref[part, cols] = running
            after = after + running[SPAN - 1 :, :]
            keys.append((gates[part] * jnp.exp(after - running)).astype(bf16))
        keys = jnp.concatenate(keys[::-1], axis=0)
        packed_ref[step * per + i, :HEAD_DIM, :] = dot(value_ref[:, cols], keys, TN).astype(bf16)
        packed_ref[step * per + i, HEAD_DIM:, :] = pack_decay(jnp.exp(after))


def local_kernel(first_ref, tp_ref, query_ref, forget_ref, value_ref, running_ref, gap_ref, local_ref, reach_ref):
    rows = query_ref.shape[0]
    row = lax.broadcasted_iota(jnp.int32, (SPAN, SPAN), 0)
    causal = lax.broadcasted_iota(jnp.int32, (SPAN, SPAN), 1) <= row
    for i in range(query_ref.shape[1] // HEAD_DIM):
        cols = slice(i * HEAD_DIM, (i + 1) * HEAD_DIM)
        before = jnp.zeros((1, HEAD_DIM), f32)
        state = None
        for start in range(0, rows, SPAN):
            part = slice(start, start + SPAN)
            logits = query_ref[part, cols].astype(f32)
            queries = logits / (1.0 + jnp.exp(-logits)) * HEAD_DIM**-0.5
            gates = input_gate(forget_ref[part, cols], gap_ref[i])
            values = value_ref[part, cols]
            running = running_ref[part, cols]
            anchor = running[SPAN // 2 - 1 : SPAN // 2, :]
            total = running[SPAN - 1 :, :]
            late = (queries * jnp.exp(running - anchor)).astype(bf16)
            early = (gates * jnp.exp(anchor - running)).astype(bf16)
            scores = jnp.where(causal, dot(late, early, NT), 0.0).astype(bf16)
            out = dot(scores, values)
            faded = queries * jnp.exp(running)
            if state is not None:
                out = out + dot(faded.astype(bf16), state.astype(bf16), NT)
            local_ref[part, cols] = out
            reach_ref[part, cols] = (faded * jnp.exp(before)).astype(bf16)
            if start + SPAN < rows:
                keys = (gates * jnp.exp(total - running)).astype(bf16)
                fresh = dot(values, keys, TN)
                state = fresh if state is None else state * jnp.exp(total) + fresh
                before = before + total


def pair_kernel(odd_ref, own_ref, other_ref, out_ref):
    even = odd_ref[0] == 0
    for head in range(own_ref.shape[0]):
        own, own_decay = unpack(own_ref, head)
        other, other_decay = unpack(other_ref, head)
        mine = jnp.where(even, other_decay, 1.0)
        theirs = jnp.where(even, 1.0, own_decay)
        out_ref[head, :HEAD_DIM, :] = (own * mine + other * theirs).astype(bf16)
        out_ref[head, HEAD_DIM:, :] = pack_decay(own_decay * other_decay)


def unpack_one_of(place, refs, head):
    parts = [unpack(ref, head) for ref in refs]
    if place is None:
        return parts[0]
    return tuple(sum(jnp.where(place == k + 1, part[i], 0.0) for k, part in enumerate(parts)) for i in range(2))


def combine_kernel(*refs, chained):
    place, refs = (refs[0][0] // 2, refs[1:]) if chained else (None, refs)
    later_ref, out_ref = refs[-2:]
    for head in range(later_ref.shape[0]):
        early, early_decay = unpack_one_of(place, refs[:-2], head)
        late, late_decay = unpack(later_ref, head)
        out_ref[head, :HEAD_DIM, :] = (early * late_decay + late).astype(bf16)
        out_ref[head, HEAD_DIM:, :] = pack_decay(early_decay * late_decay)


def carry_kernel(at_ref, *refs, chained):
    own_ref, other_ref, mine_ref, theirs_ref = refs[-4:]
    odd = at_ref[0] % 2 == 1
    place = at_ref[0] // 2 if chained else None
    for head in range(own_ref.shape[0]):
        before, _ = unpack_one_of(place, refs[:-4], head)
        own, own_decay = unpack(own_ref, head)
        other, other_decay = unpack(other_ref, head)
        first = jnp.where(odd, other, own)
        decay = jnp.where(odd, other_decay, own_decay)
        after = before * decay + first
        mine_ref[head] = jnp.where(odd, after, before).astype(bf16)
        theirs_ref[head] = jnp.where(odd, before, after).astype(bf16)


def mix_kernel(first_ref, local_ref, reach_ref, carried_ref, gate_ref, gain_ref, out_ref):
    per = out_ref.shape[1] // HEAD_DIM
    for i in range(per):
        cols = slice(i * HEAD_DIM, (i + 1) * HEAD_DIM)
        carried = carried_ref[pl.program_id(0) * per + i]
        heads_out = local_ref[:, cols] + dot(reach_ref[:, cols], carried, NT)
        mean_sq = jnp.mean(heads_out * heads_out, axis=1, keepdims=True)
        logits = gate_ref[:, cols].astype(f32)
        gates = logits / (1.0 + jnp.exp(-logits))
        mixed = heads_out * lax.rsqrt(mean_sq + epsilon) * gain_ref[...] * gates
        out_ref[:, cols] = mixed.astype(bf16)


def ring_at(place, size):
    return jnp.where(place < size // 2, 2 * place, 2 * (size - 1 - place) + 1)


def place_of(member, size):
    return jnp.where(member % 2 == 0, member // 2, size - 1 - member // 2)


def project_kernel(sp_ref, tp_ref, *refs, offsets, size, n_mixed, kept):
    mixed = refs[:n_mixed]
    chunks = refs[n_mixed : n_mixed + 2 * len(offsets)]
    table = refs[-1]
    group = (sp_ref[0] + 1 - kept) % 2
    at = place_of(sp_ref[0], size)
    half = chunks[0].shape[0]
    for i, piece in enumerate(mixed):
        table[tp_ref[0] ^ i] = piece[...]
    if kept:
        out_ref = refs[-2]
    else:
        partial_ref, out_ref, piece_ref = refs[-4:-1]
        out_ref[...] = partial_ref[...]
        piece_ref[...] = table[ring_at((at + size // 2) % size, size) // 2]

    def add(i, first):
        block = ring_at((at + (offsets[i] + size)) % size, size)

        def product():
            for start in range(0, out_ref.shape[1], TILE):
                cols = slice(start, start + TILE)
                part = dot(table[block // 2, :, :half], chunks[2 * i][:, cols])
                part = part + dot(table[block // 2, :, half:], chunks[2 * i + 1][:, cols])
                out_ref[:, cols] = part if first else out_ref[:, cols] + part

        if first:
            product()
        else:
            pl.when(block % 2 == group)(product)

    for i in range(len(offsets)):
        add(i, kept and i == 0)


def last_kernel(partial_ref, piece_ref, first_ref, second_ref, out_ref, square_ref, lanes_ref):
    half = first_ref.shape[0]
    for start in range(0, out_ref.shape[1], TILE):
        cols = slice(start, start + TILE)
        total = partial_ref[:, cols] + dot(piece_ref[:, :half], first_ref[:, cols])
        rounded = (total + dot(piece_ref[:, half:], second_ref[:, cols])).astype(bf16)
        out_ref[:, cols] = rounded
        wide = rounded.astype(f32)
        squares = wide * wide
        lanes = squares[:, :128]
        for first in range(128, TILE, 128):
            lanes = lanes + squares[:, first : first + 128]
        lanes_ref[...] = lanes if start == 0 else lanes_ref[...] + lanes
    high, low = split2(lanes_ref[...])
    ones = jnp.ones((8, 128), bf16)
    square_ref[...] = (dot(ones, high, NT) + dot(ones, low, NT))[:1]


def norm_kernel(*refs, width, count):
    squares = refs[:-6]
    projected_ref, residual_ref, gain_ref, out_ref, stage_ref, sems = refs[-6:]
    total = squares[0][...]
    for other in squares[1:]:
        total = total + other[...]
    scales = jnp.broadcast_to(lax.rsqrt(total / width + epsilon), (8, total.shape[1]))
    rows = out_ref.shape[0] // count
    copies = []
    for i in range(count):
        part = slice(i * rows, (i + 1) * rows)
        scale = jnp.transpose(scales[:, part])[:, :1]
        branch = projected_ref[part, :].astype(f32) * scale * gain_ref[...]
        stage_ref[part, :] = (residual_ref[part, :].astype(f32) + branch).astype(bf16)
        copies.append(pltpu.make_async_copy(stage_ref.at[pl.ds(i * rows, rows)], out_ref.at[pl.ds(i * rows, rows)], sems.at[i]))
        copies[-1].start()
    for copy in copies:
        copy.wait()


def vmem():
    return pl.BlockSpec(memory_space=pltpu.VMEM)


def smem():
    return pl.BlockSpec(memory_space=pltpu.SMEM)


def resident(array):
    return pltpu.with_memory_space_constraint(array, pltpu.VMEM)


def outside(array):
    return pltpu.with_memory_space_constraint(array, pltpu.HBM)


def small(kernel, scalars, operands, outs, scratch=()):
    return pl.pallas_call(
        kernel,
        out_shape=tuple(pltpu.VMEM(*out) for out in outs),
        in_specs=[smem()] * len(scalars) + [vmem()] * len(operands),
        out_specs=tuple(vmem() for _ in outs),
        scratch_shapes=list(scratch),
        compiler_params=ROOM,
    )(*scalars, *[resident(array) for array in operands])


def call(kernel, scalars, operands, out_shape, grid, in_specs, out_specs, scratch=()):
    spec = pltpu.PrefetchScalarGridSpec(
        num_scalar_prefetch=len(scalars),
        grid=grid,
        in_specs=in_specs,
        out_specs=out_specs,
        scratch_shapes=list(scratch),
    )
    return pl.pallas_call(kernel, grid_spec=spec, out_shape=out_shape, compiler_params=ROOM)(*scalars, *operands)


def is_ringed(sp, tp):
    return sp == 2 * tp and sp <= 8


def ring_gather(halves, axis):
    size = lax.axis_size(axis)
    ring = list(range(0, size, 2)) + list(range(1, size, 2))[::-1]
    forward = [(ring[i], ring[(i + 1) % size]) for i in range(size)]
    backward = [(b, a) for a, b in forward]
    chunks = {0: halves}
    for step in range(1, size // 2):
        chunks[-step], chunks[step] = [None, None], [None, None]
        for part in range(2):
            for sign, pairs, half in ((-1, forward, part), (1, backward, 1 - part)):
                chunks[sign * step][half] = lax.ppermute(chunks[sign * (step - 1)][half], axis, pairs)
    last = size // 2
    chunks[last] = (lax.ppermute(chunks[1 - last][0], axis, forward), lax.ppermute(chunks[last - 1][1], axis, backward))
    return chunks


def swap(array, axis, bit):
    size = lax.axis_size(axis)
    return lax.ppermute(array, axis, [(i, i ^ bit) for i in range(size)])


def shift(array, axis, by):
    size = lax.axis_size(axis)
    return lax.ppermute(array, axis, [(i, i + by) for i in range(size - by)])


def carried_states(given, kept, axis, at):
    size = lax.axis_size(axis)
    other = swap(given, axis, 1)
    (pair,) = small(pair_kernel, (at % 2,), (kept, other), [(kept.shape, bf16)])

    members = size // 2
    chained = members <= 4

    def combine(earlier, later):
        return small(
            functools.partial(combine_kernel, chained=chained),
            (at,) * chained,
            (*earlier, later),
            [(later.shape, bf16)],
        )[0]

    if chained:
        before = []
        for place in range(members - 1):
            sent = combine(before, pair) if before else pair
            pairs = [(2 * place + i, 2 * place + 2 + i) for i in range(2)]
            before.append(lax.ppermute(sent, axis, pairs))
    else:
        earlier, later, reach = shift(pair, axis, 2), None, 2
        while reach < members:
            before = earlier if later is None else combine([earlier], later)
            earlier, later = shift(combine([before], pair), axis, 2 * reach), before
            reach *= 2
        before = [combine([earlier], later)]
    state = ((kept.shape[0], HEAD_DIM, HEAD_DIM), bf16)
    carry = functools.partial(carry_kernel, chained=chained)
    mine, theirs = small(carry, (at,), (*before, kept, other), [state, state])
    return mine, swap(theirs, axis, 1)


def layer(
    query_logits,
    forget_logits,
    value_inputs,
    output_gate_logits,
    forget_floor_gap,
    surge_log_decay,
    head_norm_gain,
    output_matrix,
    branch_norm_gain,
    residual,
):
    rows, head_cols = query_logits.shape
    heads = head_cols // HEAD_DIM
    sp, tp = lax.axis_size("sp"), lax.axis_size("tp")
    sp_at = lax.axis_index("sp").astype(jnp.int32).reshape(1)
    tp_at = lax.axis_index("tp").astype(jnp.int32).reshape(1)
    odd = sp_at % 2
    width = output_matrix.shape[0] * sp
    out_cols = output_matrix.shape[1]
    ringed = is_ringed(sp, tp)

    group = heads // 2
    per = 2
    steps = group // per
    gap = forget_floor_gap.reshape(-1, 1, HEAD_DIM)
    block = pl.BlockSpec((rows, per * HEAD_DIM), lambda s, first, at: (0, first[0] + s))
    own_block = pl.BlockSpec((rows, per * HEAD_DIM), lambda s, first, at: (0, s))
    gap_block = pl.BlockSpec((per, 1, HEAD_DIM), lambda s, first, at: (at[0] * (heads // per) + first[0] + s, 0, 0))
    wide = jax.ShapeDtypeStruct((rows, group * HEAD_DIM), f32)
    narrow = jax.ShapeDtypeStruct((rows, group * HEAD_DIM), bf16)

    def group_states(first, place=lambda array: array):
        return call(
            states_kernel,
            (first, tp_at),
            [place(array) for array in (forget_logits, value_inputs, surge_log_decay, gap)],
            (wide, pltpu.VMEM((group, HEAD_DIM + EXTRA, HEAD_DIM), bf16)),
            (steps,),
            [block, block, pl.BlockSpec((heads, rows), lambda s, first, at: (0, 0)), gap_block],
            (own_block, vmem()),
            [pltpu.VMEM((rows, heads), f32)],
        )

    def group_local(first, running):
        return call(
            local_kernel,
            (first, tp_at),
            (query_logits, forget_logits, value_inputs, running, gap),
            (wide, narrow),
            (steps,),
            [block, block, block, own_block, gap_block],
            (own_block, own_block),
        )

    def group_mix(first, local, reach, carried):
        shared = pl.BlockSpec((rows, per * HEAD_DIM), lambda s, first: (0, s))
        return call(
            mix_kernel,
            (first,),
            (local, reach, resident(carried), output_gate_logits, head_norm_gain.reshape(1, HEAD_DIM)),
            narrow,
            (steps,),
            [
                shared,
                shared,
                vmem(),
                pl.BlockSpec((rows, per * HEAD_DIM), lambda s, first: (0, first[0] + s)),
                pl.BlockSpec((1, HEAD_DIM), lambda s, first: (0, 0)),
            ],
            shared,
        )

    given_first, kept_first = (1 - odd) * steps, odd * steps
    given_running, given = group_states(given_first)
    if ringed:
        halves = pl.pallas_call(
            halves_kernel,
            out_shape=(pltpu.VMEM((output_matrix.shape[0] // 2, out_cols), bf16),) * 2,
            in_specs=[pl.BlockSpec(memory_space=pl.ANY)],
            out_specs=(vmem(), vmem()),
            scratch_shapes=[pltpu.SemaphoreType.DMA((2,))],
            compiler_params=ROOM,
            name="halves",
        )(outside(output_matrix))
        chunks = ring_gather(halves, "sp")
    else:
        whole_weight = lax.all_gather(output_matrix, "sp", axis=0, tiled=True)
    kept_running, kept = group_states(kept_first)
    mine, others = carried_states(given, kept, "sp", sp_at)
    kept_local = group_local(kept_first, kept_running)
    given_local = group_local(given_first, given_running)
    pieces = {0: [group_mix(kept_first, *kept_local, mine), group_mix(given_first, *given_local, others)]}
    bit = tp // 2
    while bit:
        for rel in sorted(pieces):
            pieces[rel ^ bit] = [swap(piece, "tp", bit) for piece in pieces[rel]]
        bit //= 2
    mixed = [piece for rel in range(tp) for piece in pieces[rel]]

    if ringed:
        offsets = [0] + [s * k for k in range(1, sp // 2) for s in (-1, 1)]
        columns = group * HEAD_DIM
        table = [pltpu.VMEM((tp, rows, columns), bf16)]
        partial_sum = ((rows, out_cols), f32)

        def product(kept, outs, *partial):
            places = offsets if kept else offsets[1:]
            return small(
                functools.partial(project_kernel, offsets=places, size=sp, n_mixed=tp, kept=kept),
                (sp_at, tp_at),
                (*mixed[1 - kept :: 2], *[half for off in places for half in chunks[off]], *partial),
                outs,
                table,
            )

        (partial,) = product(1, [partial_sum])
        partial, piece = product(0, [partial_sum, ((rows, columns), bf16)], partial)
        projected, squares = small(
            last_kernel,
            (),
            (partial, piece, *chunks[sp // 2]),
            [((rows, out_cols), bf16), ((1, rows), f32)],
            [pltpu.VMEM((rows, 128), f32)],
        )
    else:
        stacked = jnp.stack(mixed)
        index = jnp.arange(2 * tp, dtype=jnp.int32)
        where = ((index // 2) ^ tp_at[0]) * 2 + (index + odd[0]) % 2
        all_heads = jnp.moveaxis(stacked[where], 0, 1).reshape(rows, width)
        projected = jnp.dot(all_heads, whole_weight, preferred_element_type=f32).astype(bf16)
        branch = lax.optimization_barrier(projected).astype(f32)
        squares = jnp.sum(branch * branch, axis=1)[None]
    others = [swap(squares, "tp", rel) for rel in range(tp - 1, 0, -1)]
    count = 4
    gain = pl.BlockSpec((1, out_cols), lambda n, at: (0, at[0]))
    return call(
        lambda at, *refs: norm_kernel(*refs, width=width, count=count),
        (tp_at,),
        (*[resident(a) for a in (squares, *others, projected, residual)], branch_norm_gain.reshape(1, -1)),
        jax.ShapeDtypeStruct((rows, out_cols), bf16),
        (1,),
        [vmem()] * (tp + 2) + [gain],
        pl.BlockSpec(memory_space=pl.ANY),
        [pltpu.VMEM((rows, out_cols), bf16), pltpu.SemaphoreType.DMA((count,))],
    )


def solution(mesh):
    placed = (
        P("sp", "tp"),
        P("sp", "tp"),
        P("sp", "tp"),
        P("sp", "tp"),
        P(),
        P("tp", "sp"),
        P(),
        P("sp", "tp"),
        P(),
        P("sp", "tp"),
    )
    return jax.shard_map(layer, mesh=mesh, in_specs=placed, out_specs=P("sp", "tp"), check_vma=False)
```

```python
import functools

import jax
import jax.numpy as jnp
from jax import lax
from jax.experimental import pallas as pl
from jax.experimental.pallas import tpu as pltpu
from jax.sharding import PartitionSpec as P


HEAD_DIM = 128
SPAN = 128
EXTRA = 8
TILE = 256
ROOM = pltpu.CompilerParams(vmem_limit_bytes=32 * 2**20)
epsilon = 1e-06


f32 = jnp.float32
bf16 = jnp.bfloat16
NN = (((1,), (0,)), ((), ()))
TN = (((0,), (0,)), ((), ()))
NT = (((1,), (1,)), ((), ()))


def dot(a, b, dims=NN):
    return lax.dot_general(a, b, dims, preferred_element_type=f32)


def split2(value):
    high = value.astype(bf16)
    return high, (value - high.astype(f32)).astype(bf16)


def input_gate(forget_logits, gap):
    return gap / (1.0 + jnp.exp(forget_logits.astype(f32)))


def pack_decay(decay):
    first, _ = split2(decay)
    second, third = split2(decay - first.astype(f32))
    rows = [t.astype(f32) for t in (first, second, third)]
    row = lax.broadcasted_iota(jnp.int32, (EXTRA, decay.shape[-1]), 0)
    out = jnp.where(row == 2, rows[2], 0.0)
    return jnp.where(row == 0, rows[0], jnp.where(row == 1, rows[1], out)).astype(bf16)


def unpack(ref, head):
    state = ref[head, :HEAD_DIM, :].astype(f32)
    decay = jnp.sum(ref[head, HEAD_DIM:, :].astype(f32), axis=0, keepdims=True)
    return state, decay


def halves_kernel(matrix_ref, *refs):
    halves, sems = refs[:-1], refs[-1]
    rows = halves[0].shape[0]
    copies = []
    for i, half_ref in enumerate(halves):
        copies.append(pltpu.make_async_copy(matrix_ref.at[pl.ds(i * rows, rows)], half_ref, sems.at[i]))
        copies[-1].start()
    for copy in copies:
        copy.wait()


def states_kernel(first_ref, tp_ref, forget_ref, value_ref, surge_ref, gap_ref, running_ref, packed_ref, column_ref):
    step = pl.program_id(0)
    per = gap_ref.shape[0]
    rows = forget_ref.shape[0]

    @pl.when(step == 0)
    def _():
        column_ref[...] = jnp.transpose(surge_ref[...])

    column = lax.broadcasted_iota(jnp.int32, (SPAN, 2 * SPAN), 1) % SPAN
    lower = (column <= lax.broadcasted_iota(jnp.int32, (SPAN, 2 * SPAN), 0)).astype(bf16)
    surges = column_ref[...]
    lane = lax.broadcasted_iota(jnp.int32, surges.shape, 1)
    for i in range(per):
        cols = slice(i * HEAD_DIM, (i + 1) * HEAD_DIM)
        head = (first_ref[0] + step) * per + i
        gates = input_gate(forget_ref[:, cols], gap_ref[i])
        surge = jnp.sum(jnp.where(lane == head, surges, 0.0), axis=1, keepdims=True)
        high, low = split2(jnp.log1p(-gates) + surge)
        after = jnp.zeros((1, HEAD_DIM), f32)
        keys = []
        for start in reversed(range(0, rows, SPAN)):
            part = slice(start, start + SPAN)
            running = dot(lower, jnp.concatenate([high[part], low[part]], axis=0))
            running_ref[part, cols] = running
            after = after + running[SPAN - 1 :, :]
            keys.append((gates[part] * jnp.exp(after - running)).astype(bf16))
        keys = jnp.concatenate(keys[::-1], axis=0)
        packed_ref[step * per + i, :HEAD_DIM, :] = dot(value_ref[:, cols], keys, TN).astype(bf16)
        packed_ref[step * per + i, HEAD_DIM:, :] = pack_decay(jnp.exp(after))


def local_kernel(first_ref, tp_ref, query_ref, forget_ref, value_ref, running_ref, gap_ref, local_ref, reach_ref):
    rows = query_ref.shape[0]
    row = lax.broadcasted_iota(jnp.int32, (SPAN, SPAN), 0)
    causal = lax.broadcasted_iota(jnp.int32, (SPAN, SPAN), 1) <= row
    for i in range(query_ref.shape[1] // HEAD_DIM):
        cols = slice(i * HEAD_DIM, (i + 1) * HEAD_DIM)
        before = jnp.zeros((1, HEAD_DIM), f32)
        state = None
        for start in range(0, rows, SPAN):
            part = slice(start, start + SPAN)
            logits = query_ref[part, cols].astype(f32)
            queries = logits / (1.0 + jnp.exp(-logits)) * HEAD_DIM**-0.5
            gates = input_gate(forget_ref[part, cols], gap_ref[i])
            values = value_ref[part, cols]
            running = running_ref[part, cols]
            anchor = running[SPAN // 2 - 1 : SPAN // 2, :]
            total = running[SPAN - 1 :, :]
            late = (queries * jnp.exp(running - anchor)).astype(bf16)
            early = (gates * jnp.exp(anchor - running)).astype(bf16)
            scores = jnp.where(causal, dot(late, early, NT), 0.0).astype(bf16)
            out = dot(scores, values)
            faded = queries * jnp.exp(running)
            if state is not None:
                out = out + dot(faded.astype(bf16), state.astype(bf16), NT)
            local_ref[part, cols] = out
            reach_ref[part, cols] = (faded * jnp.exp(before)).astype(bf16)
            if start + SPAN < rows:
                keys = (gates * jnp.exp(total - running)).astype(bf16)
                fresh = dot(values, keys, TN)
                state = fresh if state is None else state * jnp.exp(total) + fresh
                before = before + total


def pair_kernel(odd_ref, own_ref, other_ref, out_ref):
    even = odd_ref[0] == 0
    for head in range(own_ref.shape[0]):
        own, own_decay = unpack(own_ref, head)
        other, other_decay = unpack(other_ref, head)
        mine = jnp.where(even, other_decay, 1.0)
        theirs = jnp.where(even, 1.0, own_decay)
        out_ref[head, :HEAD_DIM, :] = (own * mine + other * theirs).astype(bf16)
        out_ref[head, HEAD_DIM:, :] = pack_decay(own_decay * other_decay)


def unpack_one_of(place, refs, head):
    parts = [unpack(ref, head) for ref in refs]
    if place is None:
        return parts[0]
    return tuple(sum(jnp.where(place == k + 1, part[i], 0.0) for k, part in enumerate(parts)) for i in range(2))


def combine_kernel(*refs, chained):
    place, refs = (refs[0][0] // 2, refs[1:]) if chained else (None, refs)
    later_ref, out_ref = refs[-2:]
    for head in range(later_ref.shape[0]):
        early, early_decay = unpack_one_of(place, refs[:-2], head)
        late, late_decay = unpack(later_ref, head)
        out_ref[head, :HEAD_DIM, :] = (early * late_decay + late).astype(bf16)
        out_ref[head, HEAD_DIM:, :] = pack_decay(early_decay * late_decay)


def carry_kernel(at_ref, *refs, chained):
    own_ref, other_ref, mine_ref, theirs_ref = refs[-4:]
    odd = at_ref[0] % 2 == 1
    place = at_ref[0] // 2 if chained else None
    for head in range(own_ref.shape[0]):
        before, _ = unpack_one_of(place, refs[:-4], head)
        own, own_decay = unpack(own_ref, head)
        other, other_decay = unpack(other_ref, head)
        first = jnp.where(odd, other, own)
        decay = jnp.where(odd, other_decay, own_decay)
        after = before * decay + first
        mine_ref[head] = jnp.where(odd, after, before).astype(bf16)
        theirs_ref[head] = jnp.where(odd, before, after).astype(bf16)


def mix_kernel(first_ref, local_ref, reach_ref, carried_ref, gate_ref, gain_ref, out_ref):
    per = out_ref.shape[1] // HEAD_DIM
    for i in range(per):
        cols = slice(i * HEAD_DIM, (i + 1) * HEAD_DIM)
        carried = carried_ref[pl.program_id(0) * per + i]
        heads_out = local_ref[:, cols] + dot(reach_ref[:, cols], carried, NT)
        mean_sq = jnp.mean(heads_out * heads_out, axis=1, keepdims=True)
        logits = gate_ref[:, cols].astype(f32)
        gates = logits / (1.0 + jnp.exp(-logits))
        mixed = heads_out * lax.rsqrt(mean_sq + epsilon) * gain_ref[...] * gates
        out_ref[:, cols] = mixed.astype(bf16)


def ring_at(place, size):
    return jnp.where(place < size // 2, 2 * place, 2 * (size - 1 - place) + 1)


def place_of(member, size):
    return jnp.where(member % 2 == 0, member // 2, size - 1 - member // 2)


def project_kernel(sp_ref, tp_ref, *refs, offsets, size, n_mixed, kept):
    mixed = refs[:n_mixed]
    chunks = refs[n_mixed : n_mixed + 2 * len(offsets)]
    table = refs[-1]
    group = (sp_ref[0] + 1 - kept) % 2
    at = place_of(sp_ref[0], size)
    half = chunks[0].shape[0]
    for i, piece in enumerate(mixed):
        table[tp_ref[0] ^ i] = piece[...]
    if kept:
        out_ref = refs[-2]
    else:
        partial_ref, out_ref, piece_ref = refs[-4:-1]
        out_ref[...] = partial_ref[...]
        piece_ref[...] = table[ring_at((at + size // 2) % size, size) // 2]

    def add(i, first):
        block = ring_at((at + (offsets[i] + size)) % size, size)

        def product():
            for start in range(0, out_ref.shape[1], TILE):
                cols = slice(start, start + TILE)
                part = dot(table[block // 2, :, :half], chunks[2 * i][:, cols])
                part = part + dot(table[block // 2, :, half:], chunks[2 * i + 1][:, cols])
                out_ref[:, cols] = part if first else out_ref[:, cols] + part

        if first:
            product()
        else:
            pl.when(block % 2 == group)(product)

    for i in range(len(offsets)):
        add(i, kept and i == 0)


def last_kernel(partial_ref, piece_ref, first_ref, second_ref, out_ref, square_ref, lanes_ref):
    half = first_ref.shape[0]
    for start in range(0, out_ref.shape[1], TILE):
        cols = slice(start, start + TILE)
        total = partial_ref[:, cols] + dot(piece_ref[:, :half], first_ref[:, cols])
        rounded = (total + dot(piece_ref[:, half:], second_ref[:, cols])).astype(bf16)
        out_ref[:, cols] = rounded
        wide = rounded.astype(f32)
        squares = wide * wide
        lanes = squares[:, :128]
        for first in range(128, TILE, 128):
            lanes = lanes + squares[:, first : first + 128]
        lanes_ref[...] = lanes if start == 0 else lanes_ref[...] + lanes
    high, low = split2(lanes_ref[...])
    ones = jnp.ones((8, 128), bf16)
    square_ref[...] = (dot(ones, high, NT) + dot(ones, low, NT))[:1]


def norm_kernel(*refs, width, count):
    squares = refs[:-6]
    projected_ref, residual_ref, gain_ref, out_ref, stage_ref, sems = refs[-6:]
    total = squares[0][...]
    for other in squares[1:]:
        total = total + other[...]
    scales = jnp.broadcast_to(lax.rsqrt(total / width + epsilon), (8, total.shape[1]))
    rows = out_ref.shape[0] // count
    copies = []
    for i in range(count):
        part = slice(i * rows, (i + 1) * rows)
        scale = jnp.transpose(scales[:, part])[:, :1]
        branch = projected_ref[part, :].astype(f32) * scale * gain_ref[...]
        stage_ref[part, :] = (residual_ref[part, :].astype(f32) + branch).astype(bf16)
        copies.append(pltpu.make_async_copy(stage_ref.at[pl.ds(i * rows, rows)], out_ref.at[pl.ds(i * rows, rows)], sems.at[i]))
        copies[-1].start()
    for copy in copies:
        copy.wait()


def vmem():
    return pl.BlockSpec(memory_space=pltpu.VMEM)


def smem():
    return pl.BlockSpec(memory_space=pltpu.SMEM)


def resident(array):
    return pltpu.with_memory_space_constraint(array, pltpu.VMEM)


def outside(array):
    return pltpu.with_memory_space_constraint(array, pltpu.HBM)


def small(kernel, scalars, operands, outs, scratch=()):
    return pl.pallas_call(
        kernel,
        out_shape=tuple(pltpu.VMEM(*out) for out in outs),
        in_specs=[smem()] * len(scalars) + [vmem()] * len(operands),
        out_specs=tuple(vmem() for _ in outs),
        scratch_shapes=list(scratch),
        compiler_params=ROOM,
    )(*scalars, *[resident(array) for array in operands])


def call(kernel, scalars, operands, out_shape, grid, in_specs, out_specs, scratch=()):
    spec = pltpu.PrefetchScalarGridSpec(
        num_scalar_prefetch=len(scalars),
        grid=grid,
        in_specs=in_specs,
        out_specs=out_specs,
        scratch_shapes=list(scratch),
    )
    return pl.pallas_call(kernel, grid_spec=spec, out_shape=out_shape, compiler_params=ROOM)(*scalars, *operands)


def is_ringed(sp, tp):
    return sp == 2 * tp and sp <= 8


def ring_gather(halves, axis):
    size = lax.axis_size(axis)
    ring = list(range(0, size, 2)) + list(range(1, size, 2))[::-1]
    forward = [(ring[i], ring[(i + 1) % size]) for i in range(size)]
    backward = [(b, a) for a, b in forward]
    chunks = {0: halves}
    for step in range(1, size // 2):
        chunks[-step], chunks[step] = [None, None], [None, None]
        for part in range(2):
            for sign, pairs, half in ((-1, forward, part), (1, backward, 1 - part)):
                chunks[sign * step][half] = lax.ppermute(chunks[sign * (step - 1)][half], axis, pairs)
    last = size // 2
    chunks[last] = (lax.ppermute(chunks[1 - last][0], axis, forward), lax.ppermute(chunks[last - 1][1], axis, backward))
    return chunks


def swap(array, axis, bit):
    size = lax.axis_size(axis)
    return lax.ppermute(array, axis, [(i, i ^ bit) for i in range(size)])


def shift(array, axis, by):
    size = lax.axis_size(axis)
    return lax.ppermute(array, axis, [(i, i + by) for i in range(size - by)])


def carried_states(given, kept, axis, at):
    size = lax.axis_size(axis)
    other = swap(given, axis, 1)
    (pair,) = small(pair_kernel, (at % 2,), (kept, other), [(kept.shape, bf16)])

    members = size // 2
    chained = members <= 4

    def combine(earlier, later):
        return small(
            functools.partial(combine_kernel, chained=chained),
            (at,) * chained,
            (*earlier, later),
            [(later.shape, bf16)],
        )[0]

    if chained:
        before = []
        for place in range(members - 1):
            sent = combine(before, pair) if before else pair
            pairs = [(2 * place + i, 2 * place + 2 + i) for i in range(2)]
            before.append(lax.ppermute(sent, axis, pairs))
    else:
        earlier, later, reach = shift(pair, axis, 2), None, 2
        while reach < members:
            before = earlier if later is None else combine([earlier], later)
            earlier, later = shift(combine([before], pair), axis, 2 * reach), before
            reach *= 2
        before = [combine([earlier], later)]
    state = ((kept.shape[0], HEAD_DIM, HEAD_DIM), bf16)
    carry = functools.partial(carry_kernel, chained=chained)
    mine, theirs = small(carry, (at,), (*before, kept, other), [state, state])
    return mine, swap(theirs, axis, 1)


def layer(
    query_logits,
    forget_logits,
    value_inputs,
    output_gate_logits,
    forget_floor_gap,
    surge_log_decay,
    head_norm_gain,
    output_matrix,
    branch_norm_gain,
    residual,
):
    query_logits, forget_logits, value_inputs, output_gate_logits, surge_log_decay = (
        outside(a) for a in (query_logits, forget_logits, value_inputs, output_gate_logits, surge_log_decay)
    )
    rows, head_cols = query_logits.shape
    heads = head_cols // HEAD_DIM
    sp, tp = lax.axis_size("sp"), lax.axis_size("tp")
    sp_at = lax.axis_index("sp").astype(jnp.int32).reshape(1)
    tp_at = lax.axis_index("tp").astype(jnp.int32).reshape(1)
    odd = sp_at % 2
    width = output_matrix.shape[0] * sp
    out_cols = output_matrix.shape[1]
    ringed = is_ringed(sp, tp)

    group = heads // 2
    per = 4
    steps = group // per
    gap = forget_floor_gap.reshape(-1, 1, HEAD_DIM)
    block = pl.BlockSpec((rows, per * HEAD_DIM), lambda s, first, at: (0, first[0] + s))
    own_block = pl.BlockSpec((rows, per * HEAD_DIM), lambda s, first, at: (0, s))
    gap_block = pl.BlockSpec((per, 1, HEAD_DIM), lambda s, first, at: (at[0] * (heads // per) + first[0] + s, 0, 0))
    wide = jax.ShapeDtypeStruct((rows, group * HEAD_DIM), f32)
    narrow = jax.ShapeDtypeStruct((rows, group * HEAD_DIM), bf16)

    def group_states(first):
        return call(
            states_kernel,
            (first, tp_at),
            (forget_logits, value_inputs, surge_log_decay, outside(gap)),
            (wide, pltpu.VMEM((group, HEAD_DIM + EXTRA, HEAD_DIM), bf16)),
            (steps,),
            [block, block, pl.BlockSpec((heads, rows), lambda s, first, at: (0, 0)), gap_block],
            (own_block, vmem()),
            [pltpu.VMEM((rows, heads), f32)],
        )

    def group_local(first, running):
        return call(
            local_kernel,
            (first, tp_at),
            (query_logits, forget_logits, value_inputs, running, gap),
            (wide, narrow),
            (steps,),
            [block, block, block, own_block, gap_block],
            (own_block, own_block),
        )

    def group_mix(first, local, reach, carried):
        shared = pl.BlockSpec((rows, per * HEAD_DIM), lambda s, first: (0, s))
        return call(
            mix_kernel,
            (first,),
            (local, reach, resident(carried), output_gate_logits, head_norm_gain.reshape(1, HEAD_DIM)),
            narrow,
            (steps,),
            [
                shared,
                shared,
                vmem(),
                pl.BlockSpec((rows, per * HEAD_DIM), lambda s, first: (0, first[0] + s)),
                pl.BlockSpec((1, HEAD_DIM), lambda s, first: (0, 0)),
            ],
            shared,
        )

    given_first, kept_first = (1 - odd) * steps, odd * steps
    given_running, given = group_states(given_first)
    if ringed:
        halves = pl.pallas_call(
            halves_kernel,
            out_shape=(pltpu.VMEM((output_matrix.shape[0] // 2, out_cols), bf16),) * 2,
            in_specs=[pl.BlockSpec(memory_space=pl.ANY)],
            out_specs=(vmem(), vmem()),
            scratch_shapes=[pltpu.SemaphoreType.DMA((2,))],
            compiler_params=ROOM,
            name="halves",
        )(outside(output_matrix))
        chunks = ring_gather(halves, "sp")
    else:
        whole_weight = lax.all_gather(output_matrix, "sp", axis=0, tiled=True)
    kept_running, kept = group_states(kept_first)
    mine, others = carried_states(given, kept, "sp", sp_at)
    kept_local = group_local(kept_first, kept_running)
    given_local = group_local(given_first, given_running)
    pieces = {0: [group_mix(kept_first, *kept_local, mine), group_mix(given_first, *given_local, others)]}
    bit = tp // 2
    while bit:
        for rel in sorted(pieces):
            pieces[rel ^ bit] = [swap(piece, "tp", bit) for piece in pieces[rel]]
        bit //= 2
    mixed = [piece for rel in range(tp) for piece in pieces[rel]]

    if ringed:
        offsets = [0] + [s * k for k in range(1, sp // 2) for s in (-1, 1)]
        columns = group * HEAD_DIM
        table = [pltpu.VMEM((tp, rows, columns), bf16)]
        partial_sum = ((rows, out_cols), f32)

        def product(kept, outs, *partial):
            places = offsets if kept else offsets[1:]
            return small(
                functools.partial(project_kernel, offsets=places, size=sp, n_mixed=tp, kept=kept),
                (sp_at, tp_at),
                (*mixed[1 - kept :: 2], *[half for off in places for half in chunks[off]], *partial),
                outs,
                table,
            )

        (partial,) = product(1, [partial_sum])
        partial, piece = product(0, [partial_sum, ((rows, columns), bf16)], partial)
        projected, squares = small(
            last_kernel,
            (),
            (partial, piece, *chunks[sp // 2]),
            [((rows, out_cols), bf16), ((1, rows), f32)],
            [pltpu.VMEM((rows, 128), f32)],
        )
    else:
        stacked = jnp.stack(mixed)
        index = jnp.arange(2 * tp, dtype=jnp.int32)
        where = ((index // 2) ^ tp_at[0]) * 2 + (index + odd[0]) % 2
        all_heads = jnp.moveaxis(stacked[where], 0, 1).reshape(rows, width)
        projected = jnp.dot(all_heads, whole_weight, preferred_element_type=f32).astype(bf16)
        branch = lax.optimization_barrier(projected).astype(f32)
        squares = jnp.sum(branch * branch, axis=1)[None]
    others = [swap(squares, "tp", rel) for rel in range(tp - 1, 0, -1)]
    count = 4
    gain = pl.BlockSpec((1, out_cols), lambda n, at: (0, at[0]))
    return call(
        lambda at, *refs: norm_kernel(*refs, width=width, count=count),
        (tp_at,),
        (*[resident(a) for a in (squares, *others, projected, residual)], branch_norm_gain.reshape(1, -1)),
        jax.ShapeDtypeStruct((rows, out_cols), bf16),
        (1,),
        [vmem()] * (tp + 2) + [gain],
        pl.BlockSpec(memory_space=pl.ANY),
        [pltpu.VMEM((rows, out_cols), bf16), pltpu.SemaphoreType.DMA((count,))],
    )


def solution(mesh):
    placed = (
        P("sp", "tp"),
        P("sp", "tp"),
        P("sp", "tp"),
        P("sp", "tp"),
        P(),
        P("tp", "sp"),
        P(),
        P("sp", "tp"),
        P(),
        P("sp", "tp"),
    )
    step = jax.shard_map(layer, mesh=mesh, in_specs=placed, out_specs=P("sp", "tp"), check_vma=False)
    if not is_ringed(mesh.shape["sp"], mesh.shape["tp"]):
        return step
    return step
```
